32 devices in a mesh: ep: 32 (over z, y, x, core).
Axes of the slice: x: 2, y: 2, z: 4, core: 2. Of those that a mesh axis runs over, the one named last changes fastest.
Arguments:
- tokens: bfloat16 [640, 2048], P('ep'), may hold values from -6 to 6
- positions: int32 [640], P('ep'), may hold values from 1024 to 16383
- state: float32 [640, 8, 64, 128], P('ep'), may hold values from -1.6 to 1.6
- mix_gain: float32 [2048], replicated, may hold values from 0.1 to 1.9
- w_query: bfloat16 [2048, 512], replicated, may hold values from -0.125 to 0.125
- w_key: bfloat16 [2048, 512], replicated, may hold values from -0.125 to 0.125
- w_value: bfloat16 [2048, 1024], replicated, may hold values from -0.125 to 0.125
- ret_gain: float32 [1024], replicated, may hold values from 0.1 to 1.9
- w_out: bfloat16 [1024, 2048], P(None, 'ep'), may hold values from -0.1875 to 0.1875
- ffn_gain: float32 [2048], replicated, may hold values from 0.1 to 1.9
- routes: int32 [640, 6], P('ep'), may hold values from 0 to 31, all different within a row; in each aligned block of 20 rows (0 to 19, 20 to 39, ...) at most 7 rows name the same one
- route_weights: float32 [640, 6], P('ep'), may hold values from 0.1 to 1
- expert_gate: bfloat16 [32, 2048, 512], P('ep'), may hold values from -0.125 to 0.125
- expert_up: bfloat16 [32, 2048, 512], P('ep'), may hold values from -0.125 to 0.125
- expert_down: bfloat16 [32, 512, 2048], P('ep'), may hold values from -0.25 to 0.25
Outputs:
- result: bfloat16 [640, 2048], P('ep')
- new_state: float32 [640, 8, 64, 128], P('ep')
The draws below stay inside these ranges and needn't reach their ends.
Inputs may be any that keep to these rules, and one draw needn't show every extreme that they name: `routes`: each row names 6 different experts; among the rows of one device no expert is named more than 7 times, a bound that some block reaches there.
All inputs are finite; a program needn't handle non-finite values.
Results may differ from the reference program's by a relative error of at most 0.017.
Values may be sent and summed in bfloat16 or wider, within the bound.
A program may use at most 128 MiB of HBM per device.

```python
import math
import jax
import jax.numpy as jnp
import numpy as np
from jax import lax

D = 2048
HEADS = 8
HEAD_K = 64
HEAD_V = 128
FE = 512
TOPK = 6
SEQ_DEV = 20
QK = 512
VW = 1024
EXPERTS = 32
CAP = 7
TOKENS = 640
N_EP = 32


def touch_ends(values, own_key, smallest, top_value):
    longest = values.shape.index(max(values.shape))
    spots = []
    for shift in (0, 1):
        where = [jax.random.randint(jax.random.fold_in(own_key, axis), (), 0, length) for axis, length in enumerate(values.shape)]
        where[longest] = (where[longest] + shift) % values.shape[longest]
        spots.append(tuple(where))
    return values.at[spots[0]].set(smallest).at[spots[1]].set(top_value)


def shard_levels(rng, extent, pieces, smallest, high):
    level = 1.0
    for dim, blocks in pieces:
        heights = jax.random.uniform(jax.random.fold_in(jax.random.fold_in(rng, 6), dim), (blocks,), jnp.float32, smallest / len(pieces), high / len(pieces))
        level = level * jnp.repeat(jnp.exp(heights), extent[dim] // blocks).reshape((-1,) + (1,) * (len(extent) - 1 - dim))
    return level


def assign_block(stream_key, own, number, rows, count, top, bound, skew):
    order = jax.random.permutation(stream_key, count)
    crowded, common = portions_of(count, rows * top, bound, skew, True), portions_of(count, rows * top, bound, skew, False)
    places = jnp.arange(count)

    def named(sizes, rotation):
        used = int((sizes > 0).sum())
        fixed = max(1, used // 4)
        passed = fixed + (places - fixed + rotation * (used - fixed)) % max(1, count - fixed)
        return jnp.zeros((count,), jnp.int32).at[order[jnp.where(places < fixed, places, passed)]].set(jnp.asarray(sizes, jnp.int32))

    sizes = jnp.where(number % 4 == 0, named(crowded, number // 4), named(common, number - number // 4 - 1))
    mixed = jax.random.permutation(jax.random.fold_in(own, 3), count)
    donor, receiver = mixed[0:count // 2 * 2:2], mixed[1:count // 2 * 2:2]
    margin = jnp.minimum(sizes[donor] - 1, bound - sizes[receiver]) // 2
    margin = jnp.where((donor == order[0]) | (receiver == order[0]) | (sizes[receiver] == 0), 0, jnp.maximum(margin, 0))
    passed = jax.random.randint(jax.random.fold_in(own, 4), (count // 2,), 0, 1 << 20) % (margin + 1)
    sizes = sizes.at[donor].add(-passed).at[receiver].add(passed)
    items = jnp.searchsorted(jnp.cumsum(sizes), jnp.arange(rows * top), side="right").astype(jnp.int32)
    listing = items.reshape(top, rows).T
    listing = listing[jax.random.permutation(jax.random.fold_in(own, 1), rows)]
    rotation = jax.random.randint(jax.random.fold_in(own, 2), (rows, 1), 0, top)
    return jnp.take_along_axis(listing, (jnp.arange(top)[None, :] + rotation) % top, axis=1)


def portions_of(amount, total, limit, lean, full):
    weights = [(1 << 20) // math.isqrt(standing ** lean) + 1 for standing in range(1, amount + 1)]
    largest = limit if full else min(limit, max(-(-total // amount), total * weights[0] // sum(weights)))
    least = 1 if total - largest >= amount - 1 else 0
    given, spare = [largest] + [least] * (amount - 1), total - largest - least * (amount - 1)
    while spare > 0:
        free = [i for i in range(1, amount) if given[i] < largest] or [i for i in range(1, amount) if given[i] < limit]
        mass, remaining = sum([weights[i] for i in free]), spare
        for i in free:
            extra = min(limit - given[i], max(1, remaining * weights[i] // mass), spare)
            given[i] = given[i] + extra
            spare = spare - extra
    return np.array(given)


def bell_draw(key, shape, spread, reach, cuts=(), held_as=jnp.bfloat16):
    values = jax.random.normal(key, shape, jnp.float32) * spread
    if len(cuts) > 0:
        values = shard_levels(key, shape, cuts, -0.22, 0.18) * values
    return jnp.clip(values, min=-reach, max=reach).astype(held_as)


def setup_inputs(seed: int = 0) -> dict:
    key_list = jax.random.split(jax.random.key(seed), 16)
    tokens = bell_draw(key_list[0], (TOKENS, D), 1.0, 6.0, ((0, 32),))
    positions = touch_ends(jax.random.randint(key_list[1], (TOKENS,), 1024, 16384), jax.random.fold_in(key_list[1], 1), 1024, 16383).astype(jnp.int32)
    state = bell_draw(key_list[2], (TOKENS, HEADS, HEAD_K, HEAD_V), 0.2, 1.6, ((0, 32),), jnp.float32)
    mix_gain = jnp.clip(1.0 + 0.18 * jax.random.normal(key_list[3], (D,), jnp.float32), 0.1, 1.9)
    w_query = bell_draw(key_list[4], (D, QK), D ** -0.5, 0.125)
    w_key = bell_draw(key_list[5], (D, QK), D ** -0.5, 0.125)
    w_value = bell_draw(key_list[6], (D, VW), D ** -0.5, 0.125)
    ret_gain = jnp.clip(1.0 + 0.18 * jax.random.normal(key_list[7], (VW,), jnp.float32), 0.1, 1.9)
    w_out = bell_draw(key_list[8], (VW, D), VW ** -0.5, 0.1875, ((1, 32),))
    ffn_gain = jnp.clip(1.0 + 0.18 * jax.random.normal(key_list[9], (D,), jnp.float32), 0.1, 1.9)
    routes_keys = jax.random.split(jax.random.fold_in(key_list[10], 1), TOKENS // SEQ_DEV)
    routes_turns = jax.random.permutation(jax.random.fold_in(key_list[10], 3), TOKENS // SEQ_DEV)
    routes = jax.vmap(lambda own, number: assign_block(jax.random.fold_in(key_list[10], 2), own, number, SEQ_DEV, EXPERTS, TOPK, CAP, 1))(routes_keys, routes_turns).reshape((TOKENS, TOPK))
    route_weights = jnp.clip(0.1 + 0.9 * jax.random.uniform(key_list[11], (TOKENS, TOPK), jnp.float32) ** shard_levels(key_list[11], (TOKENS, TOPK), ((0, 32),), -0.2, 0.2), 0.1, 1.0)
    expert_gate = bell_draw(key_list[12], (EXPERTS, D, FE), D ** -0.5, 0.125, ((0, 32),))
    expert_up = bell_draw(key_list[13], (EXPERTS, D, FE), D ** -0.5, 0.125, ((0, 32),))
    expert_down = bell_draw(key_list[14], (EXPERTS, FE, D), FE ** -0.5, 0.25, ((0, 32),))
    return {"tokens": tokens, "positions": positions, "state": state, "mix_gain": mix_gain, "w_query": w_query, "w_key": w_key, "w_value": w_value, "ret_gain": ret_gain, "w_out": w_out, "ffn_gain": ffn_gain, "routes": routes, "route_weights": route_weights, "expert_gate": expert_gate, "expert_up": expert_up, "expert_down": expert_down}


EPS = 1e-06

def rms_scale(values, gain):
    wide = values.astype(jnp.float32)
    scaled = wide * lax.rsqrt(lax.optimization_barrier(jnp.mean(wide * wide, axis=-1, keepdims=True)) + EPS)
    return (scaled * gain.astype(jnp.float32)).astype(jnp.bfloat16)

def rotate(field, spots):
    half = field.shape[-1] // 2
    freqs = jnp.exp(-math.log(10000.0) * jnp.arange(half, dtype=jnp.float32) / half)
    angle = spots.astype(jnp.float32)[:, None] * freqs[None, :]
    cosine = jnp.cos(angle)[:, None, :]
    sine = jnp.sin(angle)[:, None, :]
    first = field[..., :half]
    second = field[..., half:]
    return jnp.concatenate([first * cosine - second * sine, second * cosine + first * sine], axis=-1)

def reference(tokens, positions, state, mix_gain, w_query, w_key, w_value, ret_gain, w_out, ffn_gain, routes, route_weights, expert_gate, expert_up, expert_down):
    normed_in = rms_scale(tokens, mix_gain)
    q_proj = jnp.dot(normed_in, w_query, preferred_element_type=jnp.float32).astype(jnp.bfloat16)
    k_proj = jnp.dot(normed_in, w_key, preferred_element_type=jnp.float32).astype(jnp.bfloat16)
    v_proj = jnp.dot(normed_in, w_value, preferred_element_type=jnp.float32).astype(jnp.bfloat16)
    queries = rotate(q_proj.astype(jnp.float32).reshape(TOKENS, HEADS, HEAD_K), positions)
    key_rows = rotate(k_proj.astype(jnp.float32).reshape(TOKENS, HEADS, HEAD_K), positions) * HEAD_K ** (-0.5)
    values = v_proj.astype(jnp.float32).reshape(TOKENS, HEADS, HEAD_V)
    decays = 1.0 - jnp.exp2(-2.0 - jnp.arange(HEADS, dtype=jnp.float32))
    new_state = decays[None, :, None, None] * state + key_rows[:, :, :, None] * values[:, :, None, :]
    readout = jnp.einsum('thd,thdv->thv', queries, new_state, precision=lax.Precision.HIGHEST)
    centre = lax.optimization_barrier(jnp.mean(readout, axis=-1, keepdims=True))
    variance = lax.optimization_barrier(jnp.mean(jnp.square(readout - centre), axis=-1, keepdims=True))
    normed = ((readout - centre) * lax.rsqrt(variance + EPS)).reshape(TOKENS, VW) * ret_gain
    mixed = normed.astype(jnp.bfloat16)
    attended = jnp.dot(mixed, w_out, preferred_element_type=jnp.float32).astype(jnp.bfloat16)
    resid = (tokens.astype(jnp.float32) + attended.astype(jnp.float32)).astype(jnp.bfloat16)
    normed_mid = rms_scale(resid, ffn_gain)
    per_dev = SEQ_DEV * TOPK
    chosen = routes.reshape(N_EP, per_dev).astype(jnp.int32)
    matches = (chosen[:, :, None] == jnp.arange(EXPERTS, dtype=jnp.int32)[None, None, :]).astype(jnp.int32)
    places = lax.optimization_barrier(jnp.sum((jnp.cumsum(matches, axis=1) - matches) * matches, axis=-1))
    dev_ids = jnp.arange(N_EP, dtype=jnp.int32)[:, None]
    targets = (chosen * (N_EP * CAP) + dev_ids * CAP + places).reshape(-1).astype(jnp.int32)
    row_ids = jnp.arange(TOKENS * TOPK, dtype=jnp.int32)
    table = jnp.full((EXPERTS * N_EP * CAP,), -1, jnp.int32).at[targets].set(row_ids)
    table = table.reshape(EXPERTS, N_EP * CAP)

    def serve(items):
        gate_w, up_w, down_w, ids = items
        picked = jnp.where(ids[:, None] >= 0, normed_mid[jnp.maximum(ids, 0) // TOPK], jnp.zeros((), jnp.bfloat16))
        picked = picked.astype(jnp.bfloat16)
        gate_part = jnp.dot(picked, gate_w, preferred_element_type=jnp.float32)
        up_part = jnp.dot(picked, up_w, preferred_element_type=jnp.float32)
        hidden = (jax.nn.silu(gate_part) * up_part).astype(jnp.bfloat16)
        return jnp.dot(hidden, down_w, preferred_element_type=jnp.float32).astype(jnp.bfloat16)
    outputs = lax.map(serve, (expert_gate, expert_up, expert_down, table))
    picked_rows = outputs.reshape(-1, D)[targets].astype(jnp.float32)
    mixture = lax.optimization_barrier(jnp.sum(picked_rows.reshape(TOKENS, TOPK, D) * route_weights[:, :, None], axis=1))
    result = (resid.astype(jnp.float32) + mixture).astype(jnp.bfloat16)
    return (result, new_state)
```

```python
import functools
import math

import jax
import jax.numpy as jnp
from jax import lax
from jax.experimental import pallas as pl
from jax.experimental.pallas import tpu as pltpu
from jax.sharding import PartitionSpec as P

EPS = 1e-06
MESH = pl.DeviceIdType.MESH
PAD = 8
VMEM_LIMIT = 64 * 1024 * 1024 - 128 * 1024


def layout_of(mesh):
    devices = list(mesh.devices.flat)
    count = len(devices)
    try:
        far = [max(d.coords[i] for d in devices) - min(d.coords[i] for d in devices) + 1 for i in range(3)]
        cores = count // (far[0] * far[1] * far[2])
        if cores * far[0] * far[1] * far[2] == count and cores >= 1:
            return (far[2], far[1], far[0], cores)
    except (AttributeError, TypeError, IndexError):
        pass
    cores = 2 if count % 2 == 0 else 1
    chips = count // cores
    side = 1
    while (side * 2) ** 2 * 4 <= chips and chips % ((side * 2) ** 2) == 0:
        side *= 2
    return (chips // (side * side), side, side, cores)


class Place:
    def __init__(self, dims):
        self.dims = dims
        depth, rows, cols, cores = dims
        me = lax.axis_index("ep")
        self.me = me
        self.spot = (
            me // (rows * cols * cores),
            (me // (cols * cores)) % rows,
            (me // cores) % cols,
            me % cores,
        )

    def at(self, dz, dy, dx, dc=0):
        total = 0
        for size, here, move in zip(self.dims, self.spot, (dz, dy, dx, dc)):
            total = total * size + self.moved(size, here, move)
        return total

    @staticmethod
    def moved(size, here, move):
        if not move % size:
            return here
        if size & (size - 1):
            return (here + move) % size
        bit = 1
        there = here
        while bit < size:
            if abs(move) & bit:
                there = there + bit - 2 * bit * ((here // bit) % 2)
            bit *= 2
        return there

    def greet(self, corners=False):
        depth, rows, cols, cores = self.dims
        moves = [(d, 0, 0, 0) for d in range(1, depth)]
        moves += [(0, d, 0, 0) for d in range(1, rows)]
        moves += [(0, 0, d, 0) for d in range(1, cols)]
        if corners:
            moves += [(0, dy, dx, 0) for dy in range(1, rows) for dx in range(1, cols)]
        moves += [(0, 0, 0, d) for d in range(1, cores)]
        barrier = pltpu.get_barrier_semaphore()
        for move in moves:
            pl.semaphore_signal(barrier, inc=1, device_id=(self.at(*move),), device_id_type=MESH)
        pl.semaphore_wait(barrier, len(moves))


def bits_of(number):
    return [1 << b for b in range(number.bit_length()) if number >> b & 1]


def relay_bit(depth, dz):
    if depth & (depth - 1) or len(bits_of(dz)) < 2:
        return 0
    return bits_of(dz)[0]


def gather_names(dims):
    depth, rows, cols, cores = dims
    names = []
    for dz in range(depth):
        if dz:
            names.append(("z", dz, 0, 0, 0))
        for dx in range(1, cols):
            names.append(("x", dz, 0, dx, 0))
        for dy in range(1, rows):
            names.append(("y", dz, dy, 0, 0))
            for dx in range(1, cols):
                names.append(("p", dz, dy, dx, 0))
                names.append(("q", dz, dy, dx, 0))
        for dy in range(rows):
            for dx in range(cols):
                for dc in range(1, cores):
                    names.append(("c", dz, dy, dx, dc))
    return {name: i for i, name in enumerate(names)}


class Gather:
    def __init__(self, place, view, send, recv, split=True):
        self.place, self.view, self.send, self.recv = place, view, send, recv
        self.names = gather_names(place.dims)
        self.parts = {"p": 0, "q": 1} if split else {"p": None}
        self.sent = []

    def copy(self, name):
        kind, dz, dy, dx, dc = name
        m = self.names[name]
        bit = relay_bit(self.place.dims[0], dz)
        back = {"z": (-(bit or dz), 0, 0, 0), "x": (0, 0, -dx, 0), "y": (0, -dy, 0, 0)}
        back.update({"p": (0, -dy, 0, 0), "q": (0, 0, -dx, 0), "c": (0, 0, 0, -dc)})
        return m, self.parts.get(kind), self.place.at(*back[kind])

    def put(self, name, held):
        m, half, target = self.copy(name)
        ref = self.view(self.place.at(*held), half)
        c = pltpu.make_async_remote_copy(
            src_ref=ref, dst_ref=ref, send_sem=self.send.at[m], recv_sem=self.recv.at[m],
            device_id=(target,), device_id_type=MESH,
        )
        c.start()
        self.sent.append(c)

    def get(self, name):
        m, half, target = self.copy(name)
        ref = self.view(self.place.at(*name[1:]), half)
        pltpu.make_async_remote_copy(
            src_ref=ref, dst_ref=ref, send_sem=self.send.at[m], recv_sem=self.recv.at[m],
            device_id=(target,), device_id_type=MESH,
        ).wait_recv()

    def mates(self, dz, dy, dx):
        for dc in range(1, self.place.dims[3]):
            self.put(("c", dz, dy, dx, dc), (dz, dy, dx, 0))

    def away(self):
        depth = self.place.dims[0]
        for d in range(1, depth):
            if not relay_bit(depth, d):
                self.put(("z", d, 0, 0, 0), (0, 0, 0, 0))

    def arrive(self, dz):
        depth = self.place.dims[0]
        self.get(("z", dz, 0, 0, 0))
        for d in range(1, depth):
            bit = relay_bit(depth, d)
            if bit and d ^ bit == dz:
                self.put(("z", d, 0, 0, 0), (dz, 0, 0, 0))

    def first(self, dz):
        depth, rows, cols, cores = self.place.dims
        if dz:
            self.arrive(dz)
        else:
            self.away()
        for dx in range(1, cols):
            self.put(("x", dz, 0, dx, 0), (dz, 0, 0, 0))
        for dy in range(1, rows):
            self.put(("y", dz, dy, 0, 0), (dz, 0, 0, 0))
        self.mates(dz, 0, 0)

    def second(self, dz):
        depth, rows, cols, cores = self.place.dims
        for dx in range(1, cols):
            self.get(("x", dz, 0, dx, 0))
            for dy in range(1, rows):
                self.put(("p", dz, dy, dx, 0), (dz, 0, dx, 0))
            self.mates(dz, 0, dx)
        for dy in range(1, rows):
            self.get(("y", dz, dy, 0, 0))
            for dx in range(1, cols):
                if "q" in self.parts:
                    self.put(("q", dz, dy, dx, 0), (dz, dy, 0, 0))
            self.mates(dz, dy, 0)

    def third(self, dz):
        depth, rows, cols, cores = self.place.dims
        for dy in range(1, rows):
            for dx in range(1, cols):
                for kind in self.parts:
                    self.get((kind, dz, dy, dx, 0))
                self.mates(dz, dy, dx)

    def fourth(self, dz):
        depth, rows, cols, cores = self.place.dims
        for dy in range(rows):
            for dx in range(cols):
                for dc in range(1, cores):
                    self.get(("c", dz, dy, dx, dc))

    def finish(self):
        for c in self.sent:
            c.wait_send()


def halves(ref, width):
    cut = -(-width // 256) * 128
    spans = {None: (0, width), 0: (0, cut), 1: (cut, width - cut)}

    def view(index, half):
        start, size = spans[half]
        return ref.at[index, :, pl.ds(start, size)]

    return view


def slot_names(dims):
    kept = [name for name in gather_names(dims) if name[0] != "q"]
    table = {name: i for i, name in enumerate(kept)}
    table.update({("q",) + name[1:]: i for name, i in table.items() if name[0] == "p"})
    return table, len(kept)


class Reduce:
    def __init__(self, place, parts, slots, send, recv):
        self.place, self.parts, self.slots, self.send, self.recv = place, parts, slots, send, recv
        self.names = gather_names(place.dims)
        self.places, _ = slot_names(place.dims)
        self.sent = []
        self.width = parts.shape[2]

    def span(self, half):
        cut = self.width // 2
        return {None: pl.ds(0, self.width), 0: pl.ds(0, cut), 1: pl.ds(cut, self.width - cut)}[half]

    def copy(self, name):
        kind, dz, dy, dx, dc = name
        m = self.names[name]
        ahead = {"z": (dz, 0, 0, 0), "x": (0, 0, dx, 0), "y": (0, dy, 0, 0)}
        ahead.update({"p": (0, dy, 0, 0), "q": (0, 0, dx, 0), "c": (0, 0, 0, dc)})
        cols = self.span({"p": 0, "q": 1}.get(kind))
        return pltpu.make_async_remote_copy(
            src_ref=self.parts.at[self.place.at(dz, dy, dx, dc), :, cols],
            dst_ref=self.slots.at[self.places[name], :, cols],
            send_sem=self.send.at[m], recv_sem=self.recv.at[m],
            device_id=(self.place.at(*ahead[kind]),), device_id_type=MESH,
        )

    def put(self, name):
        c = self.copy(name)
        c.start()
        self.sent.append(c)

    def get(self, name):
        kind = name[0]
        self.copy(name).wait_recv()
        cols = self.span({"p": 0, "q": 1}.get(kind))
        return self.slots[self.places[name], :, cols].astype(jnp.float32)

    def add(self, index, cols, terms):
        value = self.parts[index, :, cols].astype(jnp.float32)
        for term in terms:
            value = value + term
        self.parts[index, :, cols] = value.astype(self.parts.dtype)

    def order(self):
        depth, rows, cols, cores = self.place.dims
        return sorted(((dy, dx) for dy in range(rows) for dx in range(cols)), key=lambda o: (not o[0]) + (not o[1]))

    def zeroth(self, dz):
        for dy, dx in self.order():
            for dc in range(1, self.place.dims[3]):
                self.put(("c", dz, dy, dx, dc))

    def first(self, dz):
        for dy, dx in self.order():
            terms = [self.get(("c", dz, dy, dx, dc)) for dc in range(1, self.place.dims[3])]
            if terms:
                self.add(self.place.at(dz, dy, dx), self.span(None), terms)
            if dy and dx:
                self.put(("p", dz, dy, dx, 0))
                self.put(("q", dz, dy, dx, 0))

    def second(self, dz):
        depth, rows, cols, cores = self.place.dims
        for dx in range(1, cols):
            terms = [self.get(("p", dz, dy, dx, 0)) for dy in range(1, rows)]
            if terms:
                self.add(self.place.at(dz, 0, dx), self.span(0), terms)
            self.put(("x", dz, 0, dx, 0))
        for dy in range(1, rows):
            terms = [self.get(("q", dz, dy, dx, 0)) for dx in range(1, cols)]
            if terms:
                self.add(self.place.at(dz, dy, 0), self.span(1), terms)
            self.put(("y", dz, dy, 0, 0))

    def third(self, dz):
        depth, rows, cols, cores = self.place.dims
        terms = [self.get(("x", dz, 0, dx, 0)) for dx in range(1, cols)]
        terms += [self.get(("y", dz, dy, 0, 0)) for dy in range(1, rows)]
        if dz:
            if terms:
                self.add(self.place.at(dz, 0, 0), self.span(None), terms)
            self.put(("z", dz, 0, 0, 0))
            return None
        value = self.parts[self.place.me].astype(jnp.float32)
        for term in terms:
            value = value + term
        return value

    def finish(self):
        for c in self.sent:
            c.wait_send()


def line_names(dims):
    depth, rows, cols, cores = dims
    names = [("z", dz) for dz in range(1, depth)]
    names += [("c", dz, dc) for dz in range(depth) for dc in range(1, cores)]
    names += [(k, dy, dx) for k in "mr" for dy in range(rows) for dx in range(cols) if dy or dx]
    return {name: i for i, name in enumerate(names)}


def rms_scale(wide, gain):
    scaled = wide * lax.rsqrt(jnp.mean(wide * wide, axis=-1, keepdims=True) + EPS)
    return (scaled * gain).astype(jnp.bfloat16)


def layer_kernel(
    dims, sizes, tokens_hbm, spots_hbm, routes_hbm, shares_hbm, gains_hbm, ret_hbm, mids_hbm, own, wq_hbm, wk_hbm, wv_hbm,
    state_hbm, gate_hbm, up_hbm, down_hbm,
    out, state,
    tokens, spots, routes, shares, gains, rets, mids, lanes_i, lanes_f,
    wq, wk, wv, flip, qcols, kcols, values, decay, readout, lines, mixed, attended, back,
    held, scales, parts, slots, gate, up, down, resid, blend, stage, share,
    load, wload, sload, send, recv, gsend, grecv, wsend, wrecv, rsend, rrecv,
):
    heads, head_k, head_v, topk = sizes
    place = Place(dims)
    seqs, width = tokens.shape
    padded = -(-seqs // PAD) * PAD
    depth, rows, cols, cores = dims
    count = math.prod(dims)
    plane = rows * cols * cores
    names = line_names(dims)

    def slot(dz, dc):
        return place.moved(depth, place.spot[0], dz) * cores + place.moved(cores, place.spot[3], dc)

    def remote(name, src, dst, target):
        m = names[name]
        return pltpu.make_async_remote_copy(
            src_ref=src, dst_ref=dst, send_sem=send.at[m], recv_sem=recv.at[m],
            device_id=(place.at(*target),), device_id_type=MESH,
        )

    pairs = [
        (own, lines.at[slot(0, 0)]), (tokens_hbm, tokens), (spots_hbm, spots), (routes_hbm, routes),
        (shares_hbm, shares), (gains_hbm, gains), (ret_hbm, rets), (mids_hbm, mids),
    ]
    fills = [pltpu.make_async_copy(a, b, load.at[i]) for i, (a, b) in enumerate(pairs)]
    for fill in fills:
        fill.start()
    weights = [
        pltpu.make_async_copy(src, dst, wload.at[i])
        for i, (src, dst) in enumerate(
            [(wq_hbm, wq), (wk_hbm, wk), (wv_hbm, wv), (gate_hbm.at[0], gate), (up_hbm.at[0], up), (down_hbm.at[0], down)]
        )
    ]
    for copy in weights[:3]:
        copy.start()
    taken = pltpu.make_async_copy(state_hbm, state, sload)
    taken.start()
    for copy in weights[3:]:
        copy.start()
    place.greet(corners=True)
    sent = []

    def put(*args):
        copy = remote(*args)
        copy.start()
        sent.append(copy)

    def line_target(dz):
        return (-(relay_bit(depth, dz) or dz), 0, 0, 0)

    def line_arrive(dz):
        ref = lines.at[slot(dz, 0)]
        remote(("z", dz), ref, ref, line_target(dz)).wait_recv()
        for d in range(1, depth):
            bit = relay_bit(depth, d)
            if bit and d ^ bit == dz:
                put(("z", d), ref, ref, line_target(d))
        for dc in range(1, cores):
            put(("c", dz, dc), ref, ref, (0, 0, 0, -dc))

    fills[0].wait()
    mine = lines.at[slot(0, 0)]
    for dz in range(1, depth):
        if not relay_bit(depth, dz):
            put(("z", dz), mine, mine, line_target(dz))
    for dc in range(1, cores):
        put(("c", 0, dc), mine, mine, (0, 0, 0, -dc))
    for fill in fills[1:]:
        fill.wait()

    lanes_i[...] = jnp.full(lanes_i.shape, -1, jnp.int32)
    lanes_f[...] = jnp.zeros_like(lanes_f)
    lanes_i[pl.ds(0, topk), pl.ds(0, seqs)] = routes[...]
    lanes_f[pl.ds(0, topk), pl.ds(0, seqs)] = shares[...]
    across = lanes_f.shape[1]
    tall_e = scales.shape[2]
    ids = lax.broadcasted_iota(jnp.int32, (tall_e, across), 0)
    wide_t = jnp.zeros((tall_e, across), jnp.float32)
    for k in range(topk):
        wide_t = wide_t + jnp.where(ids == lanes_i[pl.ds(k, 1), :], lanes_f[pl.ds(k, 1), :], 0.0)
    scales[place.me] = wide_t.T[:seqs]
    w = Gather(place, halves(scales, tall_e), wsend, wrecv, split=False)
    w.first(0)

    lanes_f[pl.ds(0, 1), pl.ds(0, seqs)] = spots[...].astype(jnp.float32)
    spread = jnp.broadcast_to(lanes_f[pl.ds(0, 1), :], (across, across)).T[:padded]
    half = head_k // 2
    index = (lax.broadcasted_iota(jnp.int32, (padded, across), 1) % half).astype(jnp.float32)
    angle = spread * jnp.exp(index * (-math.log(10000.0) / half))
    total = heads * head_k
    cosine = jnp.concatenate([jnp.cos(angle)] * (total // across), axis=1)[:seqs]
    sine = jnp.concatenate([jnp.sin(angle)] * (total // across), axis=1)[:seqs]
    normed = rms_scale(tokens[...].astype(jnp.float32), gains[...])

    def rotated(field):
        lane = lax.broadcasted_iota(jnp.int32, field.shape, 1) % head_k
        ahead = pltpu.roll(field, total - half, 1)
        behind = pltpu.roll(field, half, 1)
        return field * cosine + jnp.where(lane < half, -ahead, behind) * sine

    def columns(field, target):
        flip[...] = jnp.zeros_like(flip)
        flip[pl.ds(0, seqs), :] = field
        target[...] = flip[...].T

    def project(weight):
        part = jnp.dot(normed, weight[...], preferred_element_type=jnp.float32)
        return part.astype(jnp.bfloat16).astype(jnp.float32)

    weights[0].wait()
    columns(rotated(project(wq)), qcols)
    weights[1].wait()
    columns(rotated(project(wk)) * head_k ** (-0.5), kcols)
    weights[2].wait()
    part = project(wv)
    for h in range(heads):
        values[:, h, :] = part[:, h * head_v : (h + 1) * head_v]
        decay[pl.ds(h * head_k, head_k), :] = jnp.full((head_k, head_v), 1.0 - 2.0 ** (-2.0 - h), jnp.float32)
    w.second(0)
    taken.wait()

    def one(t, carry):
        lane = lax.broadcasted_iota(jnp.int32, qcols.shape, 1)
        query = jnp.sum(jnp.where(lane == t, qcols[...], 0.0), axis=1, keepdims=True)
        key = jnp.sum(jnp.where(lane == t, kcols[...], 0.0), axis=1, keepdims=True)
        value = values[t]
        outer = key.reshape(heads, head_k, 1) * value.reshape(heads, 1, head_v)
        fresh = decay[...] * state[t] + outer.reshape(heads * head_k, head_v)
        state[t] = fresh
        readout[t] = jnp.sum((query * fresh).reshape(heads, head_k, head_v), axis=1)
        return carry

    lax.fori_loop(0, seqs, one, 0)
    for h in range(heads):
        read = readout[:, h, :]
        apart = read - jnp.mean(read, axis=1, keepdims=True)
        variance = jnp.mean(apart * apart, axis=1, keepdims=True)
        lanes = pl.ds(h * head_v, head_v)
        mixed[0, :, lanes] = (apart * lax.rsqrt(variance + EPS) * rets[:, lanes]).astype(mixed.dtype)
    moves = [(dy, dx) for dy in range(rows) for dx in range(cols)]
    for i, (dy, dx) in enumerate(moves):
        if i:
            put(("m", dy, dx), mixed.at[0], mixed.at[i], (0, -dy, -dx, 0))
    singles = [dz for dz in range(1, depth) if not relay_bit(depth, dz)]
    relays = [dz for dz in range(1, depth) if relay_bit(depth, dz)]
    for dz in singles:
        line_arrive(dz)
        w.first(dz)
    w.third(0)
    for i, (dy, dx) in enumerate(moves):
        if i:
            remote(("m", dy, dx), mixed.at[0], mixed.at[i], (0, -dy, -dx, 0)).wait_recv()
    for dz in relays:
        line_arrive(dz)
    for dz in range(depth):
        for dc in range(1, cores):
            ref = lines.at[slot(dz, dc)]
            remote(("c", dz, dc), ref, ref, (0, 0, 0, -dc)).wait_recv()
    for i in range(len(moves)):
        blend[pl.ds(i * padded, seqs), :] = mixed[i]
    product = lax.dot_general(
        blend[...],
        lines[...].reshape(-1, lines.shape[2]),
        (((1,), (1,)), ((), ())),
        preferred_element_type=jnp.float32,
    )
    for i in range(len(moves)):
        attended[i] = product[i * padded : i * padded + seqs].astype(attended.dtype)
    for i, (dy, dx) in enumerate(moves):
        if i:
            put(("r", dy, dx), attended.at[i], back.at[i], (0, dy, dx, 0))
    for dz in relays:
        w.first(dz)
    for dz in range(1, depth):
        w.second(dz)
    for i, (dy, dx) in enumerate(moves):
        if i:
            remote(("r", dy, dx), attended.at[i], back.at[i], (0, dy, dx, 0)).wait_recv()
    chunk = cores * own.shape[0]
    y_at, x_at = place.spot[1], place.spot[2]
    arranged = []
    for y in range(rows):
        for x in range(cols):
            piece = jnp.zeros(attended.shape[1:], jnp.float32)
            for i, (dy, dx) in enumerate(moves):
                hit = jnp.logical_and(place.moved(rows, y_at, -dy) == y, place.moved(cols, x_at, -dx) == x)
                source = attended[0] if i == 0 else back[i]
                piece = jnp.where(hit, source.astype(jnp.float32), piece)
            arranged.append(piece)
    joined = jnp.concatenate(
        [a[:, z * chunk : (z + 1) * chunk] for z in range(depth) for a in arranged], axis=1
    )
    kept = (tokens[...].astype(jnp.float32) + joined).astype(jnp.bfloat16)
    resid[...] = kept
    held[place.me] = rms_scale(kept.astype(jnp.float32), mids[...])

    g = Gather(place, halves(held, width), gsend, grecv)
    r = Reduce(place, parts, slots, rsend, rrecv)
    step = stage.shape[0] // padded

    def serve(dz):
        base = place.moved(depth, place.spot[0], dz) * plane
        lane = lax.broadcasted_iota(jnp.int32, (step * padded, tall_e), 1)
        for k in range(0, plane, step):
            for i in range(step):
                stage[pl.ds(i * padded, seqs), :] = held[base + k + i]
                share[pl.ds(i * padded, seqs), :] = scales[base + k + i]
            rows_in = stage[...]
            scale = jnp.sum(jnp.where(lane == place.me, share[...], 0.0), axis=1, keepdims=True)
            gate_part = jnp.dot(rows_in, gate[...], preferred_element_type=jnp.float32)
            up_part = jnp.dot(rows_in, up[...], preferred_element_type=jnp.float32)
            hidden = (gate_part * jax.nn.sigmoid(gate_part) * up_part).astype(jnp.bfloat16)
            served = jnp.dot(hidden, down[...], preferred_element_type=jnp.float32) * scale
            for i in range(step):
                parts[base + k + i] = served[i * padded : i * padded + seqs].astype(jnp.bfloat16)

    result = None
    for t in range(depth + 5):
        if t < depth:
            g.first(t)
        if t == 0:
            for dz in range(1, depth):
                w.third(dz)
            for dz in range(depth):
                w.fourth(dz)
            for copy in weights[3:]:
                copy.wait()
        if 0 <= t - 1 < depth:
            g.second(t - 1)
        if 0 <= t - 2 < depth:
            g.third(t - 2)
        if 0 <= t - 4 < depth:
            r.second(t - 4)
        if 0 <= t - 3 < depth:
            r.first(t - 3)
        if 0 <= t - 2 < depth:
            g.fourth(t - 2)
            serve(t - 2)
            r.zeroth(t - 2)
        if 0 <= t - 5 < depth:
            value = r.third(t - 5)
            result = value if value is not None else result
    for dz in range(1, depth):
        result = result + r.get(("z", dz, 0, 0, 0))
    out[...] = (resid[...].astype(jnp.float32) + result).astype(out.dtype)
    for copy in sent:
        copy.wait_send()
    w.finish()
    g.finish()
    r.finish()


def give_kernel(result, fresh, result_out, fresh_out, sems):
    copies = [
        pltpu.make_async_copy(fresh, fresh_out, sems.at[0]),
        pltpu.make_async_copy(result, result_out, sems.at[1]),
    ]
    for copy in copies:
        copy.start()
    for copy in copies:
        copy.wait()


def shards(
    dims, tokens, positions, state, mix_gain, w_query, w_key, w_value, ret_gain, w_out, ffn_gain,
    routes, route_weights, expert_gate, expert_up, expert_down,
):
    seqs, width = tokens.shape
    heads, head_k, head_v = state.shape[1:]
    topk = routes.shape[1]
    depth, rows, cols, cores = dims
    count = math.prod(dims)
    flat = (seqs, heads * head_k, head_v)
    anywhere = pl.BlockSpec(memory_space=pl.ANY)
    here = pl.BlockSpec(memory_space=pltpu.VMEM)
    across = -(-seqs // 128) * 128
    padded = -(-seqs // PAD) * PAD
    block = w_out.T
    some = depth * cores * block.shape[0]
    plane = rows * cols
    tall_e = -(-count // 128) * 128
    lines = len(line_names(dims))
    messages = len(gather_names(dims))
    step = max(1, 192 // padded)
    while (plane * cores) % step:
        step -= 1
    operands = (
        tokens, positions.reshape(1, -1), routes.T, route_weights.T, mix_gain.reshape(1, -1), ret_gain.reshape(1, -1),
        ffn_gain.reshape(1, -1), block, w_query, w_key, w_value, state.reshape(flat), expert_gate, expert_up, expert_down,
    )
    result, fresh = pl.pallas_call(
        functools.partial(layer_kernel, dims, (heads, head_k, head_v, topk)),
        out_shape=(pltpu.VMEM((seqs, width), jnp.bfloat16), pltpu.VMEM(flat, jnp.float32)),
        in_specs=[anywhere] * len(operands),
        out_specs=(here, here),
        scratch_shapes=[
            pltpu.VMEM((seqs, width), jnp.bfloat16),
            pltpu.VMEM((1, seqs), jnp.int32),
            pltpu.VMEM((topk, seqs), jnp.int32),
            pltpu.VMEM((topk, seqs), jnp.float32),
            pltpu.VMEM((1, width), jnp.float32),
            pltpu.VMEM((1, heads * head_v), jnp.float32),
            pltpu.VMEM((1, width), jnp.float32),
            pltpu.VMEM((8, across), jnp.int32),
            pltpu.VMEM((8, across), jnp.float32),
            pltpu.VMEM(w_query.shape, w_query.dtype),
            pltpu.VMEM(w_key.shape, w_key.dtype),
            pltpu.VMEM(w_value.shape, w_value.dtype),
            pltpu.VMEM((across, heads * head_k), jnp.float32),
            pltpu.VMEM((heads * head_k, across), jnp.float32),
            pltpu.VMEM((heads * head_k, across), jnp.float32),
            pltpu.VMEM((seqs, heads, head_v), jnp.float32),
            pltpu.VMEM((heads * head_k, head_v), jnp.float32),
            pltpu.VMEM((seqs, heads, head_v), jnp.float32),
            pltpu.VMEM((depth * cores,) + block.shape, block.dtype),
            pltpu.VMEM((plane, seqs, heads * head_v), jnp.bfloat16),
            pltpu.VMEM((plane, seqs, some), jnp.bfloat16),
            pltpu.VMEM((plane, seqs, some), jnp.bfloat16),
            pltpu.VMEM((count, seqs, width), jnp.bfloat16),
            pltpu.VMEM((count, seqs, tall_e), jnp.float32),
            pltpu.VMEM((count, seqs, width), jnp.bfloat16),
            pltpu.VMEM((slot_names(dims)[1], seqs, width), jnp.bfloat16),
            pltpu.VMEM(expert_gate.shape[1:], expert_gate.dtype),
            pltpu.VMEM(expert_up.shape[1:], expert_up.dtype),
            pltpu.VMEM(expert_down.shape[1:], expert_down.dtype),
            pltpu.VMEM((seqs, width), jnp.bfloat16),
            pltpu.VMEM((plane * padded, heads * head_v), jnp.bfloat16),
            pltpu.VMEM((step * padded, width), jnp.bfloat16),
            pltpu.VMEM((step * padded, tall_e), jnp.float32),
            pltpu.SemaphoreType.DMA((8,)),
            pltpu.SemaphoreType.DMA((6,)),
            pltpu.SemaphoreType.DMA,
        ] + [pltpu.SemaphoreType.DMA((lines,))] * 2 + [pltpu.SemaphoreType.DMA((messages,))] * 6,
        compiler_params=pltpu.CompilerParams(
            collective_id=0, has_side_effects=True, vmem_limit_bytes=VMEM_LIMIT - 4 * math.prod(flat) - (1 << 19)
        ),
        name="layer",
    )(*operands)
    result, fresh = pl.pallas_call(
        give_kernel,
        out_shape=(
            jax.ShapeDtypeStruct((seqs, width), jnp.bfloat16),
            jax.ShapeDtypeStruct(flat, jnp.float32),
        ),
        in_specs=[here, here],
        out_specs=(anywhere, anywhere),
        scratch_shapes=[pltpu.SemaphoreType.DMA((2,))],
        compiler_params=pltpu.CompilerParams(vmem_limit_bytes=1 << 20),
        name="give",
    )(result, fresh)
    return (result, fresh.reshape(state.shape))


def solution(mesh):
    placed = (
        P("ep", None),
        P("ep"),
        P("ep", None, None, None),
        P(),
        P(),
        P(),
        P(),
        P(),
        P(None, "ep"),
        P(),
        P("ep", None),
        P("ep", None),
        P("ep", None, None),
        P("ep", None, None),
        P("ep", None, None),
    )
    return jax.shard_map(
        functools.partial(shards, layout_of(mesh)),
        mesh=mesh,
        in_specs=placed,
        out_specs=(P("ep", None), P("ep", None, None, None)),
        check_vma=False,
    )
```

```python
import functools
import math

import jax
import jax.numpy as jnp
from jax import lax
from jax.experimental import pallas as pl
from jax.experimental.pallas import tpu as pltpu
from jax.sharding import PartitionSpec as P

EPS = 1e-06
MESH = pl.DeviceIdType.MESH
PAD = 8
VMEM_LIMIT = 64 * 1024 * 1024 - 128 * 1024


def layout_of(mesh):
    devices = list(mesh.devices.flat)
    count = len(devices)
    try:
        far = [max(d.coords[i] for d in devices) - min(d.coords[i] for d in devices) + 1 for i in range(3)]
        cores = count // (far[0] * far[1] * far[2])
        if cores * far[0] * far[1] * far[2] == count and cores >= 1:
            return (far[2], far[1], far[0], cores)
    except (AttributeError, TypeError, IndexError):
        pass
    cores = 2 if count % 2 == 0 else 1
    chips = count // cores
    side = 1
    while (side * 2) ** 2 * 4 <= chips and chips % ((side * 2) ** 2) == 0:
        side *= 2
    return (chips // (side * side), side, side, cores)


class Place:
    def __init__(self, dims):
        self.dims = dims
        depth, rows, cols, cores = dims
        me = lax.axis_index("ep")
        self.me = me
        self.spot = (
            me // (rows * cols * cores),
            (me // (cols * cores)) % rows,
            (me // cores) % cols,
            me % cores,
        )

    def at(self, dz, dy, dx, dc=0):
        total = 0
        for size, here, move in zip(self.dims, self.spot, (dz, dy, dx, dc)):
            total = total * size + self.moved(size, here, move)
        return total

    @staticmethod
    def moved(size, here, move):
        if not move % size:
            return here
        if size & (size - 1):
            return (here + move) % size
        bit = 1
        there = here
        while bit < size:
            if abs(move) & bit:
                there = there + bit - 2 * bit * ((here // bit) % 2)
            bit *= 2
        return there

    def greet(self, corners=False):
        depth, rows, cols, cores = self.dims
        moves = [(d, 0, 0, 0) for d in range(1, depth)]
        moves += [(0, d, 0, 0) for d in range(1, rows)]
        moves += [(0, 0, d, 0) for d in range(1, cols)]
        if corners:
            moves += [(0, dy, dx, 0) for dy in range(1, rows) for dx in range(1, cols)]
        moves += [(0, 0, 0, d) for d in range(1, cores)]
        barrier = pltpu.get_barrier_semaphore()
        for move in moves:
            pl.semaphore_signal(barrier, inc=1, device_id=(self.at(*move),), device_id_type=MESH)
        return len(moves)

    @staticmethod
    def met(count):
        pl.semaphore_wait(pltpu.get_barrier_semaphore(), count)


def bits_of(number):
    return [1 << b for b in range(number.bit_length()) if number >> b & 1]


def relay_bit(depth, dz):
    if depth & (depth - 1) or len(bits_of(dz)) < 2:
        return 0
    return bits_of(dz)[0]


def gather_names(dims):
    depth, rows, cols, cores = dims
    names = []
    for dz in range(depth):
        for half in range(2):
            if dz:
                names.append(("z", dz, 0, 0, 0, half))
            for dx in range(1, cols):
                names.append(("x", dz, 0, dx, 0, half))
            for dy in range(1, rows):
                names.append(("y", dz, dy, 0, 0, half))
                for dx in range(1, cols):
                    names.append(("d", dz, dy, dx, 0, half))
        for dy in range(rows):
            for dx in range(cols):
                for dc in range(1, cores):
                    names.append(("c", dz, dy, dx, dc, None))
    return {name: i for i, name in enumerate(names)}


class Gather:
    def __init__(self, place, view, send, recv, split=True):
        self.place, self.view, self.send, self.recv = place, view, send, recv
        self.direct = () if split else tuple(range(place.dims[0]))
        self.names = gather_names(place.dims)
        self.halves = (0, 1) if split else (0,)
        self.split = split
        self.sent = []

    def copy(self, name):
        kind, dz, dy, dx, dc, half = name
        m = self.names[name]
        bit = self.relay(dz)
        back = {"z": (-(bit or dz), 0, 0, 0), "x": (0, 0, -dx, 0), "y": (0, -dy, 0, 0), "c": (0, 0, 0, -dc)}
        back["d"] = (0, 0, -dx, 0) if half else (0, -dy, 0, 0)
        if dz in self.direct:
            back["d"] = (0, -dy, -dx, 0)
        return m, half if self.split else None, self.place.at(*back[kind])

    def relay(self, dz):
        return relay_bit(self.place.dims[0], dz) if self.split else 0

    def put(self, name, held):
        m, half, target = self.copy(name)
        ref = self.view(self.place.at(*held), half)
        c = pltpu.make_async_remote_copy(
            src_ref=ref, dst_ref=ref, send_sem=self.send.at[m], recv_sem=self.recv.at[m],
            device_id=(target,), device_id_type=MESH,
        )
        c.start()
        self.sent.append(c)

    def get(self, name):
        m, half, target = self.copy(name)
        ref = self.view(self.place.at(*name[1:5]), half)
        pltpu.make_async_remote_copy(
            src_ref=ref, dst_ref=ref, send_sem=self.send.at[m], recv_sem=self.recv.at[m],
            device_id=(target,), device_id_type=MESH,
        ).wait_recv()

    def mates(self, dz, dy, dx):
        for dc in range(1, self.place.dims[3]):
            self.put(("c", dz, dy, dx, dc, None), (dz, dy, dx, 0))

    def away(self):
        depth = self.place.dims[0]
        for d in reversed(range(1, depth)):
            if not self.relay(d):
                for half in self.halves:
                    self.put(("z", d, 0, 0, 0, half), (0, 0, 0, 0))

    def spread(self, dz, half):
        depth, rows, cols, cores = self.place.dims
        for dx in range(1, cols):
            self.put(("x", dz, 0, dx, 0, half), (dz, 0, 0, 0))
        for dy in range(1, rows):
            self.put(("y", dz, dy, 0, 0, half), (dz, 0, 0, 0))
        if dz in self.direct:
            for dy in range(1, rows):
                for dx in range(1, cols):
                    self.put(("d", dz, dy, dx, 0, half), (dz, 0, 0, 0))

    def first(self, dz):
        depth = self.place.dims[0]
        for half in self.halves:
            if dz:
                self.get(("z", dz, 0, 0, 0, half))
                for d in range(1, depth):
                    bit = self.relay(d)
                    if bit and d ^ bit == dz:
                        self.put(("z", d, 0, 0, 0, half), (dz, 0, 0, 0))
            self.spread(dz, half)
        self.mates(dz, 0, 0)

    def second(self, dz):
        depth, rows, cols, cores = self.place.dims
        for half in self.halves:
            for dx in range(1, cols):
                self.get(("x", dz, 0, dx, 0, half))
                if half == 0 and dz not in self.direct:
                    for dy in range(1, rows):
                        self.put(("d", dz, dy, dx, 0, 0), (dz, 0, dx, 0))
                if half == self.halves[-1]:
                    self.mates(dz, 0, dx)
            for dy in range(1, rows):
                self.get(("y", dz, dy, 0, 0, half))
                if half == 1 and dz not in self.direct:
                    for dx in range(1, cols):
                        self.put(("d", dz, dy, dx, 0, 1), (dz, dy, 0, 0))
                if half == self.halves[-1]:
                    self.mates(dz, dy, 0)

    def third(self, dz):
        depth, rows, cols, cores = self.place.dims
        for dy in range(1, rows):
            for dx in range(1, cols):
                for half in self.halves:
                    self.get(("d", dz, dy, dx, 0, half))
                self.mates(dz, dy, dx)

    def fourth(self, dz):
        depth, rows, cols, cores = self.place.dims
        for dy in range(rows):
            for dx in range(cols):
                for dc in range(1, cores):
                    self.get(("c", dz, dy, dx, dc, None))

    def finish(self):
        for c in self.sent:
            c.wait_send()


def halves(ref, width):
    cut = -(-width // 256) * 128
    spans = {None: (0, width), 0: (0, cut), 1: (cut, width - cut)}

    def view(index, half):
        start, size = spans[half]
        return ref.at[index, :, pl.ds(start, size)]

    return view


def slot_names(dims):
    table = {}
    for name in gather_names(dims):
        table.setdefault(name[:5], len(table))
    return table


class Reduce:
    def __init__(self, place, parts, slots, send, recv):
        self.place, self.parts, self.slots, self.send, self.recv = place, parts, slots, send, recv
        self.names = gather_names(place.dims)
        self.places = slot_names(place.dims)
        self.sent = []
        self.width = parts.shape[2]

    def span(self, half):
        cut = self.width // 2
        return {None: pl.ds(0, self.width), 0: pl.ds(0, cut), 1: pl.ds(cut, self.width - cut)}[half]

    def copy(self, name):
        kind, dz, dy, dx, dc, half = name
        m = self.names[name]
        ahead = {"z": (dz, 0, 0, 0), "x": (0, 0, dx, 0), "y": (0, dy, 0, 0), "c": (0, 0, 0, dc)}
        ahead["d"] = (0, 0, dx, 0) if half else (0, dy, 0, 0)
        cols = self.span(half)
        return pltpu.make_async_remote_copy(
            src_ref=self.parts.at[self.place.at(dz, dy, dx, dc), :, cols],
            dst_ref=self.slots.at[self.places[name[:5]], :, cols],
            send_sem=self.send.at[m], recv_sem=self.recv.at[m],
            device_id=(self.place.at(*ahead[kind]),), device_id_type=MESH,
        )

    def put(self, name):
        c = self.copy(name)
        c.start()
        self.sent.append(c)

    def get(self, name):
        self.copy(name).wait_recv()
        return self.slots[self.places[name[:5]], :, self.span(name[5])].astype(jnp.float32)

    def add(self, index, cols, terms):
        value = self.parts[index, :, cols].astype(jnp.float32)
        for term in terms:
            value = value + term
        self.parts[index, :, cols] = value.astype(self.parts.dtype)

    def order(self):
        depth, rows, cols, cores = self.place.dims
        return sorted(((dy, dx) for dy in range(rows) for dx in range(cols)), key=lambda o: (not o[0]) + (not o[1]))

    def zeroth(self, dz):
        for dy, dx in self.order():
            for dc in range(1, self.place.dims[3]):
                self.put(("c", dz, dy, dx, dc, None))

    def first(self, dz):
        for dy, dx in self.order():
            terms = [self.get(("c", dz, dy, dx, dc, None)) for dc in range(1, self.place.dims[3])]
            if terms:
                self.add(self.place.at(dz, dy, dx), self.span(None), terms)
            if dy and dx:
                self.put(("d", dz, dy, dx, 0, 0))
                self.put(("d", dz, dy, dx, 0, 1))
            elif dx:
                self.put(("x", dz, 0, dx, 0, 1))
            elif dy:
                self.put(("y", dz, dy, 0, 0, 0))

    def second(self, dz):
        depth, rows, cols, cores = self.place.dims
        for dx in range(1, cols):
            terms = [self.get(("d", dz, dy, dx, 0, 0)) for dy in range(1, rows)]
            if terms:
                self.add(self.place.at(dz, 0, dx), self.span(0), terms)
            self.put(("x", dz, 0, dx, 0, 0))
        for dy in range(1, rows):
            terms = [self.get(("d", dz, dy, dx, 0, 1)) for dx in range(1, cols)]
            if terms:
                self.add(self.place.at(dz, dy, 0), self.span(1), terms)
            self.put(("y", dz, dy, 0, 0, 1))

    def third(self, dz):
        depth, rows, cols, cores = self.place.dims
        for half in range(2):
            terms = [self.get(("x", dz, 0, dx, 0, half)) for dx in range(1, cols)]
            terms += [self.get(("y", dz, dy, 0, 0, half)) for dy in range(1, rows)]
            if terms:
                self.add(self.place.at(dz, 0, 0), self.span(half), terms)
            if dz:
                self.put(("z", dz, 0, 0, 0, half))

    def total(self, half):
        value = self.parts[self.place.me, :, self.span(half)].astype(jnp.float32)
        for dz in range(1, self.place.dims[0]):
            value = value + self.get(("z", dz, 0, 0, 0, half))
        return value

    def finish(self):
        for c in self.sent:
            c.wait_send()


def plan(depth):
    relays = [dz for dz in range(1, depth) if relay_bit(depth, dz)]
    order = [0] + [dz for dz in reversed(range(1, depth)) if dz not in relays] + relays
    steps = []

    def say(kind, *planes):
        for dz in planes:
            if (kind, dz) not in steps:
                steps.append((kind, dz))

    say("away", 0)
    say("first", 0)
    say("second", 0)
    say("first", *[dz for dz in order[1:] if dz not in relays])
    for i, dz in enumerate(order):
        if i >= 1:
            say("second", dz)
            say("first", *relays)
            say("second", *order[i + 1 : i + 2])
        say("third", dz)
        if i >= 2:
            say("add1", order[i - 1])
        if i >= 3:
            say("add2", order[i - 2])
        say("fourth", dz)
        say("serve", dz)
    say("add1", *order[1:])
    say("add2", *order[-2:-1])
    say("add3", *order[1:-2])
    say("add1", 0)
    say("add2", *order[1:])
    say("add3", *order[1:-1])
    say("add2", 0)
    say("add3", *order[1:], 0)
    return steps


def line_names(dims):
    depth, rows, cols, cores = dims
    names = [("z", dz, half) for dz in range(1, depth) for half in range(2)]
    names += [("c", dz, dc) for dz in range(depth) for dc in range(1, cores)]
    moves = [(dy, dx) for dy in range(rows) for dx in range(cols) if dy or dx]
    names += [("m", dy, dx) for dy, dx in moves]
    names += [("r", dz, dy, dx) for dz in range(depth) for dy, dx in moves]
    return {name: i for i, name in enumerate(names)}


def rms_scale(wide, gain):
    scaled = wide * lax.rsqrt(jnp.mean(wide * wide, axis=-1, keepdims=True) + EPS)
    return (scaled * gain).astype(jnp.bfloat16)


def layer_kernel(
    dims, sizes, tokens_hbm, spots_hbm, routes_hbm, shares_hbm, gains_hbm, ret_hbm, mids_hbm, own, wq_hbm, wk_hbm, wv_hbm,
    state_hbm, gate_hbm, up_hbm, down_hbm,
    out, state,
    tokens, spots, routes, shares, gains, rets, mids, lanes_i, lanes_f,
    wq, wk, wv, flip, qcols, kcols, values, decay, readout, lines, mixed, attended, back,
    held, scales, parts, slots, gate, up, down, resid, blend, stage, share,
    load, wload, sload, send, recv, gsend, grecv, wsend, wrecv, rsend, rrecv,
):
    heads, head_k, head_v, topk = sizes
    place = Place(dims)
    seqs, width = tokens.shape
    padded = -(-seqs // PAD) * PAD
    depth, rows, cols, cores = dims
    count = math.prod(dims)
    plane = rows * cols * cores
    names = line_names(dims)

    def slot(dz, dc):
        return place.moved(depth, place.spot[0], dz) * cores + place.moved(cores, place.spot[3], dc)

    def remote(name, src, dst, target):
        m = names[name]
        return pltpu.make_async_remote_copy(
            src_ref=src, dst_ref=dst, send_sem=send.at[m], recv_sem=recv.at[m],
            device_id=(place.at(*target),), device_id_type=MESH,
        )

    pairs = [
        (own, lines.at[slot(0, 0)]), (tokens_hbm, tokens), (spots_hbm, spots), (routes_hbm, routes),
        (shares_hbm, shares), (gains_hbm, gains), (ret_hbm, rets), (mids_hbm, mids),
    ]
    fills = [pltpu.make_async_copy(a, b, load.at[i]) for i, (a, b) in enumerate(pairs)]
    for fill in fills:
        fill.start()
    weights = [
        pltpu.make_async_copy(src, dst, wload.at[i])
        for i, (src, dst) in enumerate(
            [(wq_hbm, wq), (wk_hbm, wk), (wv_hbm, wv), (gate_hbm.at[0], gate), (up_hbm.at[0], up), (down_hbm.at[0], down)]
        )
    ]
    for copy in weights[:2]:
        copy.start()
    partners = place.greet(corners=True)
    for fill in fills:
        fill.wait()
    taken = pltpu.make_async_copy(state_hbm, state, sload)
    weights[2].start()
    sent = []

    def put(*args):
        copy = remote(*args)
        copy.start()
        sent.append(copy)

    def line_target(dz):
        return (-(relay_bit(depth, dz) or dz), 0, 0, 0)

    def line_part(dz, half):
        rows_there = lines.shape[1] // 2
        return lines.at[slot(dz, 0), pl.ds(half * rows_there, rows_there)]

    def line_send(dz, half, held):
        ref = line_part(held, half)
        put(("z", dz, half), ref, ref, line_target(dz))

    def line_arrive(dz, half):
        ref = line_part(dz, half)
        remote(("z", dz, half), ref, ref, line_target(dz)).wait_recv()
        for d in range(1, depth):
            bit = relay_bit(depth, d)
            if bit and d ^ bit == dz:
                line_send(d, half, dz)

    def line_mates(dz):
        ref = lines.at[slot(dz, 0)]
        for dc in range(1, cores):
            put(("c", dz, dc), ref, ref, (0, 0, 0, -dc))

    lanes_i[...] = jnp.full(lanes_i.shape, -1, jnp.int32)
    lanes_f[...] = jnp.zeros_like(lanes_f)
    lanes_i[pl.ds(0, topk), pl.ds(0, seqs)] = routes[...]
    lanes_f[pl.ds(0, topk), pl.ds(0, seqs)] = shares[...]
    across = lanes_f.shape[1]
    tall_e = scales.shape[2]
    ids = lax.broadcasted_iota(jnp.int32, (tall_e, across), 0)
    wide_t = jnp.zeros((tall_e, across), jnp.float32)
    for k in range(topk):
        wide_t = wide_t + jnp.where(ids == lanes_i[pl.ds(k, 1), :], lanes_f[pl.ds(k, 1), :], 0.0)
    scales[place.me] = wide_t.T[:seqs]
    lanes_f[pl.ds(0, 1), pl.ds(0, seqs)] = spots[...].astype(jnp.float32)
    spread = jnp.broadcast_to(lanes_f[pl.ds(0, 1), :], (across, across)).T[:padded]
    turn = head_k // 2
    index = (lax.broadcasted_iota(jnp.int32, (padded, across), 1) % turn).astype(jnp.float32)
    angle = spread * jnp.exp(index * (-math.log(10000.0) / turn))
    total = heads * head_k
    cosine = jnp.concatenate([jnp.cos(angle)] * (total // across), axis=1)[:seqs]
    sine = jnp.concatenate([jnp.sin(angle)] * (total // across), axis=1)[:seqs]
    normed = rms_scale(tokens[...].astype(jnp.float32), gains[...])
    Place.met(partners)
    w = Gather(place, halves(scales, tall_e), wsend, wrecv, split=False)
    w.away()
    w.first(0)
    for dz in reversed(range(1, depth)):
        if not relay_bit(depth, dz):
            for half in range(2):
                line_send(dz, half, 0)
    line_mates(0)

    def rotated(field):
        lane = lax.broadcasted_iota(jnp.int32, field.shape, 1) % head_k
        ahead = pltpu.roll(field, total - turn, 1)
        behind = pltpu.roll(field, turn, 1)
        return field * cosine + jnp.where(lane < turn, -ahead, behind) * sine

    def columns(field, target):
        flip[...] = jnp.zeros_like(flip)
        flip[pl.ds(0, seqs), :] = field
        target[...] = flip[...].T

    def project(weight):
        part = jnp.dot(normed, weight[...], preferred_element_type=jnp.float32)
        return part.astype(jnp.bfloat16).astype(jnp.float32)

    singles = [dz for dz in reversed(range(1, depth)) if not relay_bit(depth, dz)]
    relays = [dz for dz in range(1, depth) if relay_bit(depth, dz)]
    weights[0].wait()
    columns(rotated(project(wq)), qcols)
    taken.start()
    weights[1].wait()
    columns(rotated(project(wk)) * head_k ** (-0.5), kcols)
    weights[2].wait()
    part = project(wv)
    for h in range(heads):
        values[:, h, :] = part[:, h * head_v : (h + 1) * head_v]
        decay[pl.ds(h * head_k, head_k), :] = jnp.full((head_k, head_v), 1.0 - 2.0 ** (-2.0 - h), jnp.float32)
    taken.wait()

    def one(t, carry):
        lane = lax.broadcasted_iota(jnp.int32, qcols.shape, 1)
        query = jnp.sum(jnp.where(lane == t, qcols[...], 0.0), axis=1, keepdims=True)
        key = jnp.sum(jnp.where(lane == t, kcols[...], 0.0), axis=1, keepdims=True)
        value = values[t]
        outer = key.reshape(heads, head_k, 1) * value.reshape(heads, 1, head_v)
        fresh = decay[...] * state[t] + outer.reshape(heads * head_k, head_v)
        state[t] = fresh
        readout[t] = jnp.sum((query * fresh).reshape(heads, head_k, head_v), axis=1)
        return carry

    lax.fori_loop(0, seqs // 2, one, 0, unroll=2)
    for dz in singles[:1]:
        line_arrive(dz, 0)
    for dz in range(1, depth):
        w.first(dz)
    for copy in weights[3:]:
        copy.start()
    lax.fori_loop(seqs // 2, seqs, one, 0, unroll=2)
    for h in range(heads):
        read = readout[:, h, :]
        apart = read - jnp.mean(read, axis=1, keepdims=True)
        variance = jnp.mean(apart * apart, axis=1, keepdims=True)
        lanes = pl.ds(h * head_v, head_v)
        mixed[0, :, lanes] = (apart * lax.rsqrt(variance + EPS) * rets[:, lanes]).astype(mixed.dtype)
    moves = [(dy, dx) for dy in range(rows) for dx in range(cols)]
    for i, (dy, dx) in enumerate(moves):
        if i:
            put(("m", dy, dx), mixed.at[0], mixed.at[i], (0, -dy, -dx, 0))
    for i, dz in enumerate(singles):
        for half in range(0 if i else 1, 2):
            line_arrive(dz, half)
        line_mates(dz)
    for dz in range(depth):
        w.second(dz)
        w.third(dz)
    for i, (dy, dx) in enumerate(moves):
        if i:
            remote(("m", dy, dx), mixed.at[0], mixed.at[i], (0, -dy, -dx, 0)).wait_recv()
    for i in range(len(moves)):
        blend[pl.ds(i * padded, seqs), :] = mixed[i]

    def attend(dz):
        at = place.moved(depth, place.spot[0], dz)
        for dc in range(1, cores):
            ref = lines.at[slot(dz, dc)]
            remote(("c", dz, dc), ref, ref, (0, 0, 0, -dc)).wait_recv()
        product = lax.dot_general(
            blend[...],
            lines[pl.ds(at * cores, cores)].reshape(-1, lines.shape[2]),
            (((1,), (1,)), ((), ())),
            preferred_element_type=jnp.float32,
        )
        for i, (dy, dx) in enumerate(moves):
            attended[at, i] = product[i * padded : i * padded + seqs].astype(attended.dtype)
            if i:
                put(("r", dz, dy, dx), attended.at[at, i], back.at[at, i], (0, dy, dx, 0))

    for dz in relays:
        for half in range(2):
            line_arrive(dz, half)
        line_mates(dz)
    for dz in [0] + singles + relays:
        attend(dz)
    for dz in [0] + singles + relays:
        at = place.moved(depth, place.spot[0], dz)
        for i, (dy, dx) in enumerate(moves):
            if i:
                remote(("r", dz, dy, dx), attended.at[at, i], back.at[at, i], (0, dy, dx, 0)).wait_recv()
    y_at, x_at = place.spot[1], place.spot[2]
    pieces = []
    for z in range(depth):
        found = [(attended if i == 0 else back)[z, i].astype(jnp.float32) for i in range(len(moves))]
        for y in range(rows):
            for x in range(cols):
                piece = found[0]
                for i, (dy, dx) in enumerate(moves):
                    hit = jnp.logical_and(place.moved(rows, y_at, -dy) == y, place.moved(cols, x_at, -dx) == x)
                    piece = jnp.where(hit, found[i], piece)
                pieces.append(piece)
    joined = jnp.concatenate(pieces, axis=1)
    kept = (tokens[...].astype(jnp.float32) + joined).astype(jnp.bfloat16)
    resid[...] = kept
    held[place.me] = rms_scale(kept.astype(jnp.float32), mids[...])

    g = Gather(place, halves(held, width), gsend, grecv)
    r = Reduce(place, parts, slots, rsend, rrecv)
    step = stage.shape[0] // padded

    def serve(dz):
        base = place.moved(depth, place.spot[0], dz) * plane
        lane = lax.broadcasted_iota(jnp.int32, (step * padded, tall_e), 1)
        for k in range(0, plane, step):
            for i in range(step):
                stage[pl.ds(i * padded, seqs), :] = held[base + k + i]
                share[pl.ds(i * padded, seqs), :] = scales[base + k + i]
            rows_in = stage[...]
            scale = jnp.sum(jnp.where(lane == place.me, share[...], 0.0), axis=1, keepdims=True)
            gate_part = jnp.dot(rows_in, gate[...], preferred_element_type=jnp.float32)
            up_part = jnp.dot(rows_in, up[...], preferred_element_type=jnp.float32)
            hidden = (gate_part * jax.nn.sigmoid(gate_part) * up_part).astype(jnp.bfloat16)
            served = jnp.dot(hidden, down[...], preferred_element_type=jnp.float32) * scale
            for i in range(step):
                parts[base + k + i] = served[i * padded : i * padded + seqs].astype(jnp.bfloat16)

    for kind, dz in plan(depth):
        if kind == "serve":
            if dz == 0:
                for other in range(depth):
                    w.fourth(other)
                for copy in weights[3:]:
                    copy.wait()
            serve(dz)
            r.zeroth(dz)
        else:
            act = {
                "away": lambda _: g.away(), "first": g.first, "second": g.second, "third": g.third,
                "fourth": g.fourth, "add1": r.first, "add2": r.second, "add3": r.third,
            }
            act[kind](dz)
    for half in range(2):
        cols_at = r.span(half)
        out[:, cols_at] = (resid[:, cols_at].astype(jnp.float32) + r.total(half)).astype(out.dtype)
    for copy in sent:
        copy.wait_send()
    w.finish()
    g.finish()
    r.finish()


def give_kernel(result, fresh, result_out, fresh_out, sems):
    copies = [
        pltpu.make_async_copy(fresh, fresh_out, sems.at[0]),
        pltpu.make_async_copy(result, result_out, sems.at[1]),
    ]
    for copy in copies:
        copy.start()
    for copy in copies:
        copy.wait()


def shards(
    dims, tokens, positions, state, mix_gain, w_query, w_key, w_value, ret_gain, w_out, ffn_gain,
    routes, route_weights, expert_gate, expert_up, expert_down,
):
    seqs, width = tokens.shape
    heads, head_k, head_v = state.shape[1:]
    topk = routes.shape[1]
    depth, rows, cols, cores = dims
    count = math.prod(dims)
    flat = (seqs, heads * head_k, head_v)
    anywhere = pl.BlockSpec(memory_space=pl.ANY)
    here = pl.BlockSpec(memory_space=pltpu.VMEM)
    across = -(-seqs // 128) * 128
    padded = -(-seqs // PAD) * PAD
    block = w_out.T
    some = depth * cores * block.shape[0]
    plane = rows * cols
    tall_e = -(-count // 128) * 128
    lines = len(line_names(dims))
    messages = len(gather_names(dims))
    step = max(1, 192 // padded)
    while (plane * cores) % step:
        step -= 1
    operands = (
        tokens, positions.reshape(1, -1), routes.T, route_weights.T, mix_gain.reshape(1, -1), ret_gain.reshape(1, -1),
        ffn_gain.reshape(1, -1), block, w_query, w_key, w_value, state.reshape(flat), expert_gate, expert_up, expert_down,
    )
    result, fresh = pl.pallas_call(
        functools.partial(layer_kernel, dims, (heads, head_k, head_v, topk)),
        out_shape=(pltpu.VMEM((seqs, width), jnp.bfloat16), pltpu.VMEM(flat, jnp.float32)),
        in_specs=[anywhere] * len(operands),
        out_specs=(here, here),
        scratch_shapes=[
            pltpu.VMEM((seqs, width), jnp.bfloat16),
            pltpu.VMEM((1, seqs), jnp.int32),
            pltpu.VMEM((topk, seqs), jnp.int32),
            pltpu.VMEM((topk, seqs), jnp.float32),
            pltpu.VMEM((1, width), jnp.float32),
            pltpu.VMEM((1, heads * head_v), jnp.float32),
            pltpu.VMEM((1, width), jnp.float32),
            pltpu.VMEM((8, across), jnp.int32),
            pltpu.VMEM((8, across), jnp.float32),
            pltpu.VMEM(w_query.shape, w_query.dtype),
            pltpu.VMEM(w_key.shape, w_key.dtype),
            pltpu.VMEM(w_value.shape, w_value.dtype),
            pltpu.VMEM((across, heads * head_k), jnp.float32),
            pltpu.VMEM((heads * head_k, across), jnp.float32),
            pltpu.VMEM((heads * head_k, across), jnp.float32),
            pltpu.VMEM((seqs, heads, head_v), jnp.float32),
            pltpu.VMEM((heads * head_k, head_v), jnp.float32),
            pltpu.VMEM((seqs, heads, head_v), jnp.float32),
            pltpu.VMEM((depth * cores,) + block.shape, block.dtype),
            pltpu.VMEM((plane, seqs, heads * head_v), jnp.bfloat16),
            pltpu.VMEM((depth, plane, seqs, some // depth), jnp.bfloat16),
            pltpu.VMEM((depth, plane, seqs, some // depth), jnp.bfloat16),
            pltpu.VMEM((count, seqs, width), jnp.bfloat16),
            pltpu.VMEM((count, seqs, tall_e), jnp.float32),
            pltpu.VMEM((count, seqs, width), jnp.bfloat16),
            pltpu.VMEM((len(slot_names(dims)), seqs, width), jnp.bfloat16),
            pltpu.VMEM(expert_gate.shape[1:], expert_gate.dtype),
            pltpu.VMEM(expert_up.shape[1:], expert_up.dtype),
            pltpu.VMEM(expert_down.shape[1:], expert_down.dtype),
            pltpu.VMEM((seqs, width), jnp.bfloat16),
            pltpu.VMEM((plane * padded, heads * head_v), jnp.bfloat16),
            pltpu.VMEM((step * padded, width), jnp.bfloat16),
            pltpu.VMEM((step * padded, tall_e), jnp.float32),
            pltpu.SemaphoreType.DMA((8,)),
            pltpu.SemaphoreType.DMA((6,)),
            pltpu.SemaphoreType.DMA,
        ] + [pltpu.SemaphoreType.DMA((lines,))] * 2 + [pltpu.SemaphoreType.DMA((messages,))] * 6,
        compiler_params=pltpu.CompilerParams(
            collective_id=0, has_side_effects=True, vmem_limit_bytes=VMEM_LIMIT - 4 * math.prod(flat) - (1 << 19)
        ),
        name="layer",
    )(*operands)
    result, fresh = pl.pallas_call(
        give_kernel,
        out_shape=(
            jax.ShapeDtypeStruct((seqs, width), jnp.bfloat16),
            jax.ShapeDtypeStruct(flat, jnp.float32),
        ),
        in_specs=[here, here],
        out_specs=(anywhere, anywhere),
        scratch_shapes=[pltpu.SemaphoreType.DMA((2,))],
        compiler_params=pltpu.CompilerParams(vmem_limit_bytes=1 << 20),
        name="give",
    )(result, fresh)
    return (result, fresh.reshape(state.shape))


def solution(mesh):
    placed = (
        P("ep", None),
        P("ep"),
        P("ep", None, None, None),
        P(),
        P(),
        P(),
        P(),
        P(),
        P(None, "ep"),
        P(),
        P("ep", None),
        P("ep", None),
        P("ep", None, None),
        P("ep", None, None),
        P("ep", None, None),
    )
    return jax.shard_map(
        functools.partial(shards, layout_of(mesh)),
        mesh=mesh,
        in_specs=placed,
        out_specs=(P("ep", None), P("ep", None, None, None)),
        check_vma=False,
    )
```

```python
import functools
import math

import jax
import jax.numpy as jnp
from jax import lax
from jax.experimental import pallas as pl
from jax.experimental.pallas import tpu as pltpu
from jax.sharding import PartitionSpec as P

EPS = 1e-06
MESH = pl.DeviceIdType.MESH
PAD = 8
VMEM_LIMIT = 64 * 1024 * 1024 - 128 * 1024


def layout_of(mesh):
    devices = list(mesh.devices.flat)
    count = len(devices)
    try:
        far = [max(d.coords[i] for d in devices) - min(d.coords[i] for d in devices) + 1 for i in range(3)]
        cores = count // (far[0] * far[1] * far[2])
        if cores * far[0] * far[1] * far[2] == count and cores >= 1:
            return (far[2], far[1], far[0], cores)
    except (AttributeError, TypeError, IndexError):
        pass
    cores = 2 if count % 2 == 0 else 1
    chips = count // cores
    side = 1
    while (side * 2) ** 2 * 4 <= chips and chips % ((side * 2) ** 2) == 0:
        side *= 2
    return (chips // (side * side), side, side, cores)


class Place:
    def __init__(self, dims):
        self.dims = dims
        depth, rows, cols, cores = dims
        me = lax.axis_index("ep")
        self.me = me
        self.spot = (
            me // (rows * cols * cores),
            (me // (cols * cores)) % rows,
            (me // cores) % cols,
            me % cores,
        )

    def at(self, dz, dy, dx, dc=0):
        total = 0
        for size, here, move in zip(self.dims, self.spot, (dz, dy, dx, dc)):
            total = total * size + self.moved(size, here, move)
        return total

    @staticmethod
    def moved(size, here, move):
        if not move % size:
            return here
        if size & (size - 1):
            return (here + move) % size
        bit = 1
        there = here
        while bit < size:
            if abs(move) & bit:
                there = there + bit - 2 * bit * ((here // bit) % 2)
            bit *= 2
        return there

    def greet(self, corners=False):
        depth, rows, cols, cores = self.dims
        moves = [(d, 0, 0, 0) for d in range(1, depth)]
        moves += [(0, d, 0, 0) for d in range(1, rows)]
        moves += [(0, 0, d, 0) for d in range(1, cols)]
        if corners:
            moves += [(0, dy, dx, 0) for dy in range(1, rows) for dx in range(1, cols)]
        moves += [(0, 0, 0, d) for d in range(1, cores)]
        barrier = pltpu.get_barrier_semaphore()
        for move in moves:
            pl.semaphore_signal(barrier, inc=1, device_id=(self.at(*move),), device_id_type=MESH)
        return len(moves)

    @staticmethod
    def met(count):
        pl.semaphore_wait(pltpu.get_barrier_semaphore(), count)


def bits_of(number):
    return [1 << b for b in range(number.bit_length()) if number >> b & 1]


def relay_bit(depth, dz):
    if depth & (depth - 1) or len(bits_of(dz)) < 2:
        return 0
    return bits_of(dz)[0]


def gather_names(dims):
    depth, rows, cols, cores = dims
    names = []
    for dz in range(depth):
        for half in range(2):
            if dz:
                names.append(("z", dz, 0, 0, 0, half))
            for dx in range(1, cols):
                names.append(("x", dz, 0, dx, 0, half))
            for dy in range(1, rows):
                names.append(("y", dz, dy, 0, 0, half))
                for dx in range(1, cols):
                    names.append(("d", dz, dy, dx, 0, half))
        for dy in range(rows):
            for dx in range(cols):
                for dc in range(1, cores):
                    names.append(("c", dz, dy, dx, dc, None))
    return {name: i for i, name in enumerate(names)}


class Gather:
    def __init__(self, place, view, send, recv, split=True):
        self.place, self.view, self.send, self.recv = place, view, send, recv
        singles, relays = stages(place.dims[0])
        self.direct = tuple(singles[:1] + relays) if split else tuple(range(place.dims[0]))
        self.names = gather_names(place.dims)
        self.halves = (0, 1) if split else (0,)
        self.split = split
        self.sent = []

    def copy(self, name):
        kind, dz, dy, dx, dc, half = name
        m = self.names[name]
        bit = self.relay(dz)
        back = {"z": (-(bit or dz), 0, 0, 0), "x": (0, 0, -dx, 0), "y": (0, -dy, 0, 0), "c": (0, 0, 0, -dc)}
        back["d"] = (0, 0, -dx, 0) if half else (0, -dy, 0, 0)
        if dz in self.direct:
            back["d"] = (0, -dy, -dx, 0)
        return m, half if self.split else None, self.place.at(*back[kind])

    def relay(self, dz):
        return relay_bit(self.place.dims[0], dz) if self.split else 0

    def put(self, name, held):
        m, half, target = self.copy(name)
        ref = self.view(self.place.at(*held), half)
        c = pltpu.make_async_remote_copy(
            src_ref=ref, dst_ref=ref, send_sem=self.send.at[m], recv_sem=self.recv.at[m],
            device_id=(target,), device_id_type=MESH,
        )
        c.start()
        self.sent.append(c)

    def get(self, name):
        m, half, target = self.copy(name)
        ref = self.view(self.place.at(*name[1:5]), half)
        pltpu.make_async_remote_copy(
            src_ref=ref, dst_ref=ref, send_sem=self.send.at[m], recv_sem=self.recv.at[m],
            device_id=(target,), device_id_type=MESH,
        ).wait_recv()

    def mates(self, dz, dy, dx):
        for dc in range(1, self.place.dims[3]):
            self.put(("c", dz, dy, dx, dc, None), (dz, dy, dx, 0))

    def away(self):
        depth = self.place.dims[0]
        for d in reversed(range(1, depth)):
            if not self.relay(d):
                for half in self.halves:
                    self.put(("z", d, 0, 0, 0, half), (0, 0, 0, 0))

    def spread(self, dz, half):
        depth, rows, cols, cores = self.place.dims
        for dx in range(1, cols):
            self.put(("x", dz, 0, dx, 0, half), (dz, 0, 0, 0))
        for dy in range(1, rows):
            self.put(("y", dz, dy, 0, 0, half), (dz, 0, 0, 0))
        if dz in self.direct:
            for dy in range(1, rows):
                for dx in range(1, cols):
                    self.put(("d", dz, dy, dx, 0, half), (dz, 0, 0, 0))

    def first(self, dz):
        depth = self.place.dims[0]
        for half in self.halves:
            if dz:
                self.get(("z", dz, 0, 0, 0, half))
                for d in range(1, depth):
                    bit = self.relay(d)
                    if bit and d ^ bit == dz:
                        self.put(("z", d, 0, 0, 0, half), (dz, 0, 0, 0))
            self.spread(dz, half)
        self.mates(dz, 0, 0)

    def second(self, dz):
        depth, rows, cols, cores = self.place.dims
        for half in self.halves:
            for dx in range(1, cols):
                self.get(("x", dz, 0, dx, 0, half))
                if half == 0 and dz not in self.direct:
                    for dy in range(1, rows):
                        self.put(("d", dz, dy, dx, 0, 0), (dz, 0, dx, 0))
                if half == self.halves[-1]:
                    self.mates(dz, 0, dx)
            for dy in range(1, rows):
                self.get(("y", dz, dy, 0, 0, half))
                if half == 1 and dz not in self.direct:
                    for dx in range(1, cols):
                        self.put(("d", dz, dy, dx, 0, 1), (dz, dy, 0, 0))
                if half == self.halves[-1]:
                    self.mates(dz, dy, 0)

    def third(self, dz):
        depth, rows, cols, cores = self.place.dims
        for dy in range(1, rows):
            for dx in range(1, cols):
                for half in self.halves:
                    self.get(("d", dz, dy, dx, 0, half))
                self.mates(dz, dy, dx)

    def fourth(self, dz):
        depth, rows, cols, cores = self.place.dims
        for dy in range(rows):
            for dx in range(cols):
                for dc in range(1, cores):
                    self.get(("c", dz, dy, dx, dc, None))

    def finish(self):
        for c in self.sent:
            c.wait_send()


def halves(ref, width):
    cut = -(-width // 256) * 128
    spans = {None: (0, width), 0: (0, cut), 1: (cut, width - cut)}

    def view(index, half):
        start, size = spans[half]
        return ref.at[index, :, pl.ds(start, size)]

    return view


def slot_names(dims):
    table = {}
    for name in gather_names(dims):
        table.setdefault(name[:5], len(table))
    return table


class Reduce:
    def __init__(self, place, parts, slots, send, recv):
        self.place, self.parts, self.slots, self.send, self.recv = place, parts, slots, send, recv
        self.names = gather_names(place.dims)
        self.places = slot_names(place.dims)
        self.sent = []
        self.width = parts.shape[2]

    def span(self, half):
        cut = self.width // 2
        return {None: pl.ds(0, self.width), 0: pl.ds(0, cut), 1: pl.ds(cut, self.width - cut)}[half]

    def copy(self, name):
        kind, dz, dy, dx, dc, half = name
        m = self.names[name]
        ahead = {"z": (dz, 0, 0, 0), "x": (0, 0, dx, 0), "y": (0, dy, 0, 0), "c": (0, 0, 0, dc)}
        ahead["d"] = (0, 0, dx, 0) if half else (0, dy, 0, 0)
        cols = self.span(half)
        return pltpu.make_async_remote_copy(
            src_ref=self.parts.at[self.place.at(dz, dy, dx, dc), :, cols],
            dst_ref=self.slots.at[self.places[name[:5]], :, cols],
            send_sem=self.send.at[m], recv_sem=self.recv.at[m],
            device_id=(self.place.at(*ahead[kind]),), device_id_type=MESH,
        )

    def put(self, name):
        c = self.copy(name)
        c.start()
        self.sent.append(c)

    def get(self, name):
        self.copy(name).wait_recv()
        return self.slots[self.places[name[:5]], :, self.span(name[5])].astype(jnp.float32)

    def add(self, index, cols, terms):
        value = self.parts[index, :, cols].astype(jnp.float32)
        for term in terms:
            value = value + term
        self.parts[index, :, cols] = value.astype(self.parts.dtype)

    def order(self):
        depth, rows, cols, cores = self.place.dims
        return sorted(((dy, dx) for dy in range(rows) for dx in range(cols)), key=lambda o: (not o[0]) + (not o[1]))

    def zeroth(self, dz):
        for dy, dx in self.order():
            for dc in range(1, self.place.dims[3]):
                self.put(("c", dz, dy, dx, dc, None))

    def first(self, dz):
        for dy, dx in self.order():
            terms = [self.get(("c", dz, dy, dx, dc, None)) for dc in range(1, self.place.dims[3])]
            if terms:
                self.add(self.place.at(dz, dy, dx), self.span(None), terms)
            if dy and dx:
                self.put(("d", dz, dy, dx, 0, 0))
                self.put(("d", dz, dy, dx, 0, 1))
            elif dx:
                self.put(("x", dz, 0, dx, 0, 1))
            elif dy:
                self.put(("y", dz, dy, 0, 0, 0))

    def second(self, dz):
        depth, rows, cols, cores = self.place.dims
        for dx in range(1, cols):
            terms = [self.get(("d", dz, dy, dx, 0, 0)) for dy in range(1, rows)]
            if terms:
                self.add(self.place.at(dz, 0, dx), self.span(0), terms)
            self.put(("x", dz, 0, dx, 0, 0))
        for dy in range(1, rows):
            terms = [self.get(("d", dz, dy, dx, 0, 1)) for dx in range(1, cols)]
            if terms:
                self.add(self.place.at(dz, dy, 0), self.span(1), terms)
            self.put(("y", dz, dy, 0, 0, 1))

    def third(self, dz):
        depth, rows, cols, cores = self.place.dims
        for half in range(2):
            terms = [self.get(("x", dz, 0, dx, 0, half)) for dx in range(1, cols)]
            terms += [self.get(("y", dz, dy, 0, 0, half)) for dy in range(1, rows)]
            if terms:
                self.add(self.place.at(dz, 0, 0), self.span(half), terms)
            if dz:
                self.put(("z", dz, 0, 0, 0, half))

    def total(self, half):
        value = self.parts[self.place.me, :, self.span(half)].astype(jnp.float32)
        for dz in range(1, self.place.dims[0]):
            value = value + self.get(("z", dz, 0, 0, 0, half))
        return value

    def finish(self):
        for c in self.sent:
            c.wait_send()


def stages(depth):
    relays = [dz for dz in range(1, depth) if relay_bit(depth, dz)]
    return [dz for dz in reversed(range(1, depth)) if dz not in relays], relays


def plan(depth):
    singles, relays = stages(depth)
    order = [0] + singles[:1] + relays + singles[1:]
    steps = []

    def say(kind, *planes):
        for dz in planes:
            if (kind, dz) not in steps:
                steps.append((kind, dz))

    say("away", 0)
    say("first", 0)
    say("second", 0)
    say("first", *singles)
    for i, dz in enumerate(order):
        say("second", dz)
        if i == 1:
            say("first", *relays)
            say("second", *singles)
        if i == 2:
            say("third", *singles)
        if i >= 3:
            say("add2", order[i - 2])
        if i >= 2:
            say("add1", order[i - 1])
        say("third", dz)
        say("fourth", dz)
        say("serve", dz)
    say("add3", *order[1:-2])
    say("add2", *order[1:-1])
    say("add1", *order[1:], 0)
    say("add3", *order[1:-1])
    say("add2", *order[1:], 0)
    say("add3", *order[1:], 0)
    return steps


def line_names(dims):
    depth, rows, cols, cores = dims
    names = [("z", dz, half) for dz in range(1, depth) for half in range(2)]
    names += [("c", dz, dc) for dz in range(depth) for dc in range(1, cores)]
    moves = [(dy, dx) for dy in range(rows) for dx in range(cols) if dy or dx]
    names += [("m", dy, dx) for dy, dx in moves]
    names += [("r", dz, dy, dx) for dz in range(depth) for dy, dx in moves]
    return {name: i for i, name in enumerate(names)}


def rms_scale(wide, gain):
    scaled = wide * lax.rsqrt(jnp.mean(wide * wide, axis=-1, keepdims=True) + EPS)
    return (scaled * gain).astype(jnp.bfloat16)


def layer_kernel(
    dims, sizes, tokens_hbm, spots_hbm, routes_hbm, shares_hbm, gains_hbm, ret_hbm, mids_hbm, own, wq_hbm, wk_hbm, wv_hbm,
    state_hbm, gate_hbm, up_hbm, down_hbm,
    out, state,
    tokens, spots, routes, shares, gains, rets, mids, lanes_i, lanes_f,
    wq, wk, wv, flip, qcols, kcols, values, decay, readout, lines, mixed, attended, back,
    held, scales, parts, slots, gate, up, down, resid, blend, stage, share,
    load, wload, sload, send, recv, gsend, grecv, wsend, wrecv, rsend, rrecv,
):
    heads, head_k, head_v, topk = sizes
    place = Place(dims)
    seqs, width = tokens.shape
    padded = -(-seqs // PAD) * PAD
    depth, rows, cols, cores = dims
    count = math.prod(dims)
    plane = rows * cols * cores
    names = line_names(dims)

    def slot(dz, dc):
        return place.moved(depth, place.spot[0], dz) * cores + place.moved(cores, place.spot[3], dc)

    def remote(name, src, dst, target):
        m = names[name]
        return pltpu.make_async_remote_copy(
            src_ref=src, dst_ref=dst, send_sem=send.at[m], recv_sem=recv.at[m],
            device_id=(place.at(*target),), device_id_type=MESH,
        )

    pairs = [
        (own, lines.at[slot(0, 0)]), (tokens_hbm, tokens), (spots_hbm, spots), (routes_hbm, routes),
        (shares_hbm, shares), (gains_hbm, gains), (ret_hbm, rets), (mids_hbm, mids),
    ]
    fills = [pltpu.make_async_copy(a, b, load.at[i]) for i, (a, b) in enumerate(pairs)]
    for fill in fills:
        fill.start()
    weights = [
        pltpu.make_async_copy(src, dst, wload.at[i])
        for i, (src, dst) in enumerate(
            [(wq_hbm, wq), (wk_hbm, wk), (wv_hbm, wv), (gate_hbm.at[0], gate), (up_hbm.at[0], up), (down_hbm.at[0], down)]
        )
    ]
    for copy in weights[:2]:
        copy.start()
    partners = place.greet(corners=True)
    for fill in fills:
        fill.wait()
    taken = pltpu.make_async_copy(state_hbm, state, sload)
    weights[2].start()
    sent = []

    def put(*args):
        copy = remote(*args)
        copy.start()
        sent.append(copy)

    def line_target(dz):
        return (-(relay_bit(depth, dz) or dz), 0, 0, 0)

    def line_part(dz, half):
        rows_there = lines.shape[1] // 2
        return lines.at[slot(dz, 0), pl.ds(half * rows_there, rows_there)]

    def line_send(dz, half, held):
        ref = line_part(held, half)
        put(("z", dz, half), ref, ref, line_target(dz))

    def line_arrive(dz, half):
        ref = line_part(dz, half)
        remote(("z", dz, half), ref, ref, line_target(dz)).wait_recv()
        for d in range(1, depth):
            bit = relay_bit(depth, d)
            if bit and d ^ bit == dz:
                line_send(d, half, dz)

    def line_mates(dz):
        ref = lines.at[slot(dz, 0)]
        for dc in range(1, cores):
            put(("c", dz, dc), ref, ref, (0, 0, 0, -dc))

    lanes_i[...] = jnp.full(lanes_i.shape, -1, jnp.int32)
    lanes_f[...] = jnp.zeros_like(lanes_f)
    lanes_i[pl.ds(0, topk), pl.ds(0, seqs)] = routes[...]
    lanes_f[pl.ds(0, topk), pl.ds(0, seqs)] = shares[...]
    across = lanes_f.shape[1]
    tall_e = scales.shape[2]
    ids = lax.broadcasted_iota(jnp.int32, (tall_e, across), 0)
    wide_t = jnp.zeros((tall_e, across), jnp.float32)
    for k in range(topk):
        wide_t = wide_t + jnp.where(ids == lanes_i[pl.ds(k, 1), :], lanes_f[pl.ds(k, 1), :], 0.0)
    scales[place.me] = wide_t.T[:seqs]
    lanes_f[pl.ds(0, 1), pl.ds(0, seqs)] = spots[...].astype(jnp.float32)
    spread = jnp.broadcast_to(lanes_f[pl.ds(0, 1), :], (across, across)).T[:padded]
    turn = head_k // 2
    index = (lax.broadcasted_iota(jnp.int32, (padded, across), 1) % turn).astype(jnp.float32)
    angle = spread * jnp.exp(index * (-math.log(10000.0) / turn))
    total = heads * head_k
    cosine = jnp.concatenate([jnp.cos(angle)] * (total // across), axis=1)[:seqs]
    sine = jnp.concatenate([jnp.sin(angle)] * (total // across), axis=1)[:seqs]
    normed = rms_scale(tokens[...].astype(jnp.float32), gains[...])
    Place.met(partners)
    w = Gather(place, halves(scales, tall_e), wsend, wrecv, split=False)
    w.away()
    w.first(0)
    for dz in reversed(range(1, depth)):
        if not relay_bit(depth, dz):
            for half in range(2):
                line_send(dz, half, 0)
    line_mates(0)

    def rotated(field):
        lane = lax.broadcasted_iota(jnp.int32, field.shape, 1) % head_k
        ahead = pltpu.roll(field, total - turn, 1)
        behind = pltpu.roll(field, turn, 1)
        return field * cosine + jnp.where(lane < turn, -ahead, behind) * sine

    def columns(field, target):
        flip[...] = jnp.zeros_like(flip)
        flip[pl.ds(0, seqs), :] = field
        target[...] = flip[...].T

    def project(weight):
        part = jnp.dot(normed, weight[...], preferred_element_type=jnp.float32)
        return part.astype(jnp.bfloat16).astype(jnp.float32)

    singles, relays = stages(depth)
    weights[0].wait()
    columns(rotated(project(wq)), qcols)
    taken.start()
    weights[1].wait()
    columns(rotated(project(wk)) * head_k ** (-0.5), kcols)
    weights[2].wait()
    part = project(wv)
    for h in range(heads):
        values[:, h, :] = part[:, h * head_v : (h + 1) * head_v]
        decay[pl.ds(h * head_k, head_k), :] = jnp.full((head_k, head_v), 1.0 - 2.0 ** (-2.0 - h), jnp.float32)
    taken.wait()

    def one(t, carry):
        where = jnp.full(qcols.shape, t, jnp.int32)
        query = jnp.take_along_axis(qcols[...], where, axis=1, mode="promise_in_bounds")
        key = jnp.take_along_axis(kcols[...], where, axis=1, mode="promise_in_bounds")
        value = values[t]
        shape = (heads, head_k, head_v)
        outer = key.reshape(shape) * value.reshape(heads, 1, head_v)
        fresh = decay[...] * state[t] + outer.reshape(heads * head_k, head_v)
        state[t] = fresh
        readout[t] = jnp.sum((query * fresh).reshape(shape), axis=1)
        return carry

    lax.fori_loop(0, seqs // 2, one, 0, unroll=2)
    for dz in singles[:1]:
        line_arrive(dz, 0)
    for dz in range(1, depth):
        w.first(dz)
    for copy in weights[3:]:
        copy.start()
    lax.fori_loop(seqs // 2, seqs, one, 0, unroll=2)
    for h in range(heads):
        read = readout[:, h, :]
        apart = read - jnp.mean(read, axis=1, keepdims=True)
        variance = jnp.mean(apart * apart, axis=1, keepdims=True)
        lanes = pl.ds(h * head_v, head_v)
        mixed[0, :, lanes] = (apart * lax.rsqrt(variance + EPS) * rets[:, lanes]).astype(mixed.dtype)
    moves = [(dy, dx) for dy in range(rows) for dx in range(cols)]
    for i, (dy, dx) in enumerate(moves):
        if i:
            put(("m", dy, dx), mixed.at[0], mixed.at[i], (0, -dy, -dx, 0))
    for i, dz in enumerate(singles):
        for half in range(0 if i else 1, 2):
            line_arrive(dz, half)
        line_mates(dz)
    for dz in range(depth):
        w.second(dz)
        w.third(dz)
    for i, (dy, dx) in enumerate(moves):
        if i:
            remote(("m", dy, dx), mixed.at[0], mixed.at[i], (0, -dy, -dx, 0)).wait_recv()
    for i in range(len(moves)):
        blend[pl.ds(i * padded, seqs), :] = mixed[i]

    def attend(dz):
        at = place.moved(depth, place.spot[0], dz)
        for dc in range(1, cores):
            ref = lines.at[slot(dz, dc)]
            remote(("c", dz, dc), ref, ref, (0, 0, 0, -dc)).wait_recv()
        product = lax.dot_general(
            blend[...],
            lines[pl.ds(at * cores, cores)].reshape(-1, lines.shape[2]),
            (((1,), (1,)), ((), ())),
            preferred_element_type=jnp.float32,
        )
        for i, (dy, dx) in enumerate(moves):
            attended[at, i] = product[i * padded : i * padded + seqs].astype(attended.dtype)
            if i:
                put(("r", dz, dy, dx), attended.at[at, i], back.at[at, i], (0, dy, dx, 0))

    for dz in relays:
        for half in range(2):
            line_arrive(dz, half)
        line_mates(dz)
    for dz in [0] + singles + relays:
        attend(dz)
    for dz in [0] + singles + relays:
        at = place.moved(depth, place.spot[0], dz)
        for i, (dy, dx) in enumerate(moves):
            if i:
                remote(("r", dz, dy, dx), attended.at[at, i], back.at[at, i], (0, dy, dx, 0)).wait_recv()
    y_at, x_at = place.spot[1], place.spot[2]
    pieces = []
    for z in range(depth):
        found = [(attended if i == 0 else back)[z, i].astype(jnp.float32) for i in range(len(moves))]
        for y in range(rows):
            for x in range(cols):
                piece = found[0]
                for i, (dy, dx) in enumerate(moves):
                    hit = jnp.logical_and(place.moved(rows, y_at, -dy) == y, place.moved(cols, x_at, -dx) == x)
                    piece = jnp.where(hit, found[i], piece)
                pieces.append(piece)
    joined = jnp.concatenate(pieces, axis=1)
    kept = (tokens[...].astype(jnp.float32) + joined).astype(jnp.bfloat16)
    resid[...] = kept
    held[place.me] = rms_scale(kept.astype(jnp.float32), mids[...])

    g = Gather(place, halves(held, width), gsend, grecv)
    r = Reduce(place, parts, slots, rsend, rrecv)
    step = stage.shape[0] // padded

    def serve(dz):
        base = place.moved(depth, place.spot[0], dz) * plane
        lane = lax.broadcasted_iota(jnp.int32, (step * padded, tall_e), 1)
        for k in range(0, plane, step):
            for i in range(step):
                stage[pl.ds(i * padded, seqs), :] = held[base + k + i]
                share[pl.ds(i * padded, seqs), :] = scales[base + k + i]
            rows_in = stage[...]
            scale = jnp.sum(jnp.where(lane == place.me, share[...], 0.0), axis=1, keepdims=True)
            gate_part = jnp.dot(rows_in, gate[...], preferred_element_type=jnp.float32)
            up_part = jnp.dot(rows_in, up[...], preferred_element_type=jnp.float32)
            hidden = (gate_part * jax.nn.sigmoid(gate_part) * up_part).astype(jnp.bfloat16)
            served = jnp.dot(hidden, down[...], preferred_element_type=jnp.float32) * scale
            for i in range(step):
                parts[base + k + i] = served[i * padded : i * padded + seqs].astype(jnp.bfloat16)

    for kind, dz in plan(depth):
        if kind == "serve":
            if dz == 0:
                for other in range(depth):
                    w.fourth(other)
                for copy in weights[3:]:
                    copy.wait()
            serve(dz)
            r.zeroth(dz)
        else:
            act = {
                "away": lambda _: g.away(), "first": g.first, "second": g.second, "third": g.third,
                "fourth": g.fourth, "add1": r.first, "add2": r.second, "add3": r.third,
            }
            act[kind](dz)
    for half in range(2):
        cols_at = r.span(half)
        out[:, cols_at] = (resid[:, cols_at].astype(jnp.float32) + r.total(half)).astype(out.dtype)
    for copy in sent:
        copy.wait_send()
    w.finish()
    g.finish()
    r.finish()


def give_kernel(result, fresh, result_out, fresh_out, sems):
    copies = [
        pltpu.make_async_copy(fresh, fresh_out, sems.at[0]),
        pltpu.make_async_copy(result, result_out, sems.at[1]),
    ]
    for copy in copies:
        copy.start()
    for copy in copies:
        copy.wait()


def shards(
    dims, tokens, positions, state, mix_gain, w_query, w_key, w_value, ret_gain, w_out, ffn_gain,
    routes, route_weights, expert_gate, expert_up, expert_down,
):
    seqs, width = tokens.shape
    heads, head_k, head_v = state.shape[1:]
    topk = routes.shape[1]
    depth, rows, cols, cores = dims
    count = math.prod(dims)
    flat = (seqs, heads * head_k, head_v)
    anywhere = pl.BlockSpec(memory_space=pl.ANY)
    here = pl.BlockSpec(memory_space=pltpu.VMEM)
    across = -(-seqs // 128) * 128
    padded = -(-seqs // PAD) * PAD
    block = w_out.T
    some = depth * cores * block.shape[0]
    plane = rows * cols
    tall_e = -(-count // 128) * 128
    lines = len(line_names(dims))
    messages = len(gather_names(dims))
    step = max(1, 192 // padded)
    while (plane * cores) % step:
        step -= 1
    operands = (
        tokens, positions.reshape(1, -1), routes.T, route_weights.T, mix_gain.reshape(1, -1), ret_gain.reshape(1, -1),
        ffn_gain.reshape(1, -1), block, w_query, w_key, w_value, state.reshape(flat), expert_gate, expert_up, expert_down,
    )
    result, fresh = pl.pallas_call(
        functools.partial(layer_kernel, dims, (heads, head_k, head_v, topk)),
        out_shape=(pltpu.VMEM((seqs, width), jnp.bfloat16), pltpu.VMEM(flat, jnp.float32)),
        in_specs=[anywhere] * len(operands),
        out_specs=(here, here),
        scratch_shapes=[
            pltpu.VMEM((seqs, width), jnp.bfloat16),
            pltpu.VMEM((1, seqs), jnp.int32),
            pltpu.VMEM((topk, seqs), jnp.int32),
            pltpu.VMEM((topk, seqs), jnp.float32),
            pltpu.VMEM((1, width), jnp.float32),
            pltpu.VMEM((1, heads * head_v), jnp.float32),
            pltpu.VMEM((1, width), jnp.float32),
            pltpu.VMEM((8, across), jnp.int32),
            pltpu.VMEM((8, across), jnp.float32),
            pltpu.VMEM(w_query.shape, w_query.dtype),
            pltpu.VMEM(w_key.shape, w_key.dtype),
            pltpu.VMEM(w_value.shape, w_value.dtype),
            pltpu.VMEM((across, heads * head_k), jnp.float32),
            pltpu.VMEM((heads * head_k, across), jnp.float32),
            pltpu.VMEM((heads * head_k, across), jnp.float32),
            pltpu.VMEM((seqs, heads, head_v), jnp.float32),
            pltpu.VMEM((heads * head_k, head_v), jnp.float32),
            pltpu.VMEM((seqs, heads, head_v), jnp.float32),
            pltpu.VMEM((depth * cores,) + block.shape, block.dtype),
            pltpu.VMEM((plane, seqs, heads * head_v), jnp.bfloat16),
            pltpu.VMEM((depth, plane, seqs, some // depth), jnp.bfloat16),
            pltpu.VMEM((depth, plane, seqs, some // depth), jnp.bfloat16),
            pltpu.VMEM((count, seqs, width), jnp.bfloat16),
            pltpu.VMEM((count, seqs, tall_e), jnp.float32),
            pltpu.VMEM((count, seqs, width), jnp.bfloat16),
            pltpu.VMEM((len(slot_names(dims)), seqs, width), jnp.bfloat16),
            pltpu.VMEM(expert_gate.shape[1:], expert_gate.dtype),
            pltpu.VMEM(expert_up.shape[1:], expert_up.dtype),
            pltpu.VMEM(expert_down.shape[1:], expert_down.dtype),
            pltpu.VMEM((seqs, width), jnp.bfloat16),
            pltpu.VMEM((plane * padded, heads * head_v), jnp.bfloat16),
            pltpu.VMEM((step * padded, width), jnp.bfloat16),
            pltpu.VMEM((step * padded, tall_e), jnp.float32),
            pltpu.SemaphoreType.DMA((8,)),
            pltpu.SemaphoreType.DMA((6,)),
            pltpu.SemaphoreType.DMA,
        ] + [pltpu.SemaphoreType.DMA((lines,))] * 2 + [pltpu.SemaphoreType.DMA((messages,))] * 6,
        compiler_params=pltpu.CompilerParams(
            collective_id=0, has_side_effects=True, vmem_limit_bytes=VMEM_LIMIT - 4 * math.prod(flat) - (1 << 19)
        ),
        name="layer",
    )(*operands)
    result, fresh = pl.pallas_call(
        give_kernel,
        out_shape=(
            jax.ShapeDtypeStruct((seqs, width), jnp.bfloat16),
            jax.ShapeDtypeStruct(flat, jnp.float32),
        ),
        in_specs=[here, here],
        out_specs=(anywhere, anywhere),
        scratch_shapes=[pltpu.SemaphoreType.DMA((2,))],
        compiler_params=pltpu.CompilerParams(vmem_limit_bytes=1 << 20),
        name="give",
    )(result, fresh)
    return (result, fresh.reshape(state.shape))


def solution(mesh):
    placed = (
        P("ep", None),
        P("ep"),
        P("ep", None, None, None),
        P(),
        P(),
        P(),
        P(),
        P(),
        P(None, "ep"),
        P(),
        P("ep", None),
        P("ep", None),
        P("ep", None, None),
        P("ep", None, None),
        P("ep", None, None),
    )
    return jax.shard_map(
        functools.partial(shards, layout_of(mesh)),
        mesh=mesh,
        in_specs=placed,
        out_specs=(P("ep", None), P("ep", None, None, None)),
        check_vma=False,
    )
```
